512 devices in a mesh: grp: 2 (over y), tp: 16 (over z), dp: 16 (over x, core).
Axes of the slice: x: 8, y: 2, z: 16, core: 2. Of those that a mesh axis runs over, the one named last changes fastest.
The devices are a block of a 8x16x16 slice.
Arguments:
- tokens: bfloat16 [1024, 4096], P(('grp', 'tp'), 'dp'), parts along dimension 0, may hold values from -6 to 6
- lengths: int32 [256], P(('grp', 'dp')), parts along dimension 0, may hold values from 1 to 4, as said below
- norm_gain: float32 [2, 4096], P(None, 'dp'), may hold values from 0.1 to 1.9
- w_recept: bfloat16 [2, 4096, 2048], P(None, 'dp', 'tp'), may hold values from -0.09375 to 0.09375
- w_keys: bfloat16 [2, 4096, 2048], P(None, 'dp', 'tp'), may hold values from -0.09375 to 0.09375
- w_values: bfloat16 [2, 4096, 2048], P(None, 'dp', 'tp'), may hold values from -0.09375 to 0.09375
- w_decay: bfloat16 [2, 4096, 2048], P(None, 'dp', 'tp'), may hold values from -0.09375 to 0.09375
- w_rate: bfloat16 [2, 4096, 2048], P(None, 'dp', 'tp'), may hold values from -0.09375 to 0.09375
- w_gate: bfloat16 [2, 4096, 2048], P(None, 'dp', 'tp'), may hold values from -0.09375 to 0.09375
- decay_base: float32 [2, 2048], P(None, 'tp'), may hold values from -3 to 1
- group_gain: float32 [2, 2048], P(None, 'tp'), may hold values from 0.1 to 1.9
- w_out: bfloat16 [2, 2048, 4096], P(None, 'tp', 'dp'), may hold values from -0.125 to 0.125
- states: float32 [2, 256, 32, 4096], P(None, ('grp', 'dp'), 'tp'), parts along dimension 1, may hold values from -2 to 2
Outputs:
- tokens_out: bfloat16 [1024, 4096], P(('grp', 'tp'), 'dp'), parts along dimension 0
- states_out: float32 [2, 256, 32, 4096], P(None, ('grp', 'dp'), 'tp'), parts along dimension 1
The draws below stay inside these ranges and needn't reach their ends.
There are 2 independent parts, one for each index of `grp`. The reference program is written for one: setup_inputs(seed, part) draws one part's arguments, and reference() takes and returns one part's arrays. A program takes and returns all parts, laid end to end along the dimension named above; an argument that names none is the same for every part. Nothing has to cross between parts.
Inputs may be any that keep to these rules, and one draw needn't show every extreme that they name: Sequence s has its first lengths[s] of its 4 slots live; in every draw all 8 sequences of some index of dp have 4 live slots.
All inputs are finite; a program needn't handle non-finite values.
Results may differ from the reference program's by a relative error of at most 0.029.
Values may be sent and summed in bfloat16 or wider, within the bound.
No kernel may reach another device: no remote copies, remote signals or barrier semaphores. Data moves between devices by JAX's collectives and lax.ppermute only.
A program may use at most 64 MiB of HBM per device.

```python
import jax
import jax.numpy as jnp
from jax import lax

D = 4096
HEADS = 32
HEAD = 64
NEW = 4
SEQ_DEV = 8
WIDTH = 2048
SEQS = 128
TOKENS = 512


def draw_lengths(key, part):
    key_ticket = jax.random.fold_in(key, 11)
    key_block = jax.random.fold_in(key, 12)
    ticket = jax.random.randint(key_ticket, (SEQS,), 0, 100)
    length_base = 1 + (ticket >= 55).astype(jnp.int32) + (ticket >= 85).astype(jnp.int32) + (ticket >= 93).astype(jnp.int32)
    length_base = jnp.minimum(length_base, NEW)
    chosen = jax.random.randint(key_block, (), 0, SEQS // SEQ_DEV)
    owner_block = jnp.arange(SEQS, dtype=jnp.int32) // SEQ_DEV
    return jnp.where(owner_block == chosen, NEW, length_base).astype(jnp.int32)


def block_levels(key, extent, cuts, low, high):
    def one(dim, blocks):
        heights = jax.random.uniform(jax.random.fold_in(jax.random.fold_in(key, 6), dim), (blocks,), jnp.float32, low / len(cuts), high / len(cuts))
        return jnp.repeat(jnp.exp(heights), extent[dim] // blocks).reshape((-1,) + (1,) * (len(extent) - dim - 1))

    gain = one(*cuts[0])
    for cut in cuts[1:]:
        gain = gain * one(*cut)
    return gain


def scatter_about(key, shape, spread, bound, split=(), kind=jnp.bfloat16):
    drawn = spread * jax.random.normal(key, shape, jnp.float32)
    if split:
        drawn = drawn * block_levels(key, shape, split, -0.22, 0.18)
    return jnp.clip(drawn, -bound, bound).astype(kind)


def setup_inputs(seed: int = 0, part: int = 0) -> dict:
    seeds = jax.random.split(jax.random.key(seed), 14)
    part_splits = jax.random.split(jax.random.fold_in(seeds[13], part), 14)
    tokens = scatter_about(part_splits[0], (TOKENS, D), 1.0, 6.0, ((0, 16), (1, 16)))
    lengths = draw_lengths(jax.random.fold_in(jax.random.fold_in(seeds[13], part), 71), part)
    norm_gain = jnp.clip(1.0 + 0.18 * jax.random.normal(seeds[2], (2, D), jnp.float32), 0.1, 1.9)
    w_recept = scatter_about(seeds[3], (2, D, WIDTH), D ** -0.5, 0.09375, ((1, 16), (2, 16)))
    w_keys = scatter_about(seeds[4], (2, D, WIDTH), D ** -0.5, 0.09375, ((1, 16), (2, 16)))
    w_values = scatter_about(seeds[5], (2, D, WIDTH), D ** -0.5, 0.09375, ((1, 16), (2, 16)))
    w_decay = scatter_about(seeds[6], (2, D, WIDTH), D ** -0.5, 0.09375, ((1, 16), (2, 16)))
    w_rate = scatter_about(seeds[7], (2, D, WIDTH), D ** -0.5, 0.09375, ((1, 16), (2, 16)))
    w_gate = scatter_about(seeds[8], (2, D, WIDTH), D ** -0.5, 0.09375, ((1, 16), (2, 16)))
    decay_base = jnp.clip(-3.0 + 4.0 * jax.random.uniform(seeds[9], (2, WIDTH), jnp.float32) ** block_levels(seeds[9], (2, WIDTH), ((1, 16),), -0.2, 0.2), -3.0, 1.0)
    group_gain = jnp.clip(1.0 + 0.18 * jax.random.normal(seeds[10], (2, WIDTH), jnp.float32), 0.1, 1.9)
    w_out = scatter_about(seeds[11], (2, WIDTH, D), WIDTH ** -0.5, 0.125, ((1, 16), (2, 16)))
    states = scatter_about(part_splits[12], (2, SEQS, HEADS, HEAD * HEAD), 0.3, 2.0, ((1, 16), (2, 16)), jnp.float32)
    return dict(tokens=tokens, lengths=lengths, norm_gain=norm_gain, w_recept=w_recept, w_keys=w_keys, w_values=w_values, w_decay=w_decay, w_rate=w_rate, w_gate=w_gate, decay_base=decay_base, group_gain=group_gain, w_out=w_out, states=states)


norm_epsilon = 1e-06
unit_epsilon = 0.00064
group_epsilon = 0.00064

def advance(state_in, pieces, lengths, base_log, gain_vec):
    seq_count = state_in.shape[0]
    head_count = state_in.shape[1]
    head_shape = (seq_count, NEW, head_count, HEAD)
    recept, keys, values, decay_pre, rate_pre, gate_pre = [piece.astype(jnp.float32).reshape(head_shape) for piece in pieces]
    decays = jnp.exp(-jnp.exp(-jax.nn.softplus(-(base_log.reshape(head_count, HEAD) + decay_pre)) - 0.5))
    rates = jax.nn.sigmoid(rate_pre)
    unit_keys = keys * lax.rsqrt(lax.optimization_barrier(jnp.sum(keys * keys, -1, keepdims=True)) + unit_epsilon)
    memory = state_in.reshape(seq_count, head_count, HEAD, HEAD)
    live_mask = jnp.arange(NEW)[None, :] < lengths[:, None]
    readings = []
    for position in range(NEW):
        unit_now = unit_keys[:, position]
        removed = jnp.einsum('shvk,shk->shv', memory, unit_now)
        updated = memory * decays[:, position][:, :, None, :] - removed[..., None] * (unit_now * rates[:, position])[:, :, None, :] + values[:, position][..., None] * keys[:, position][:, :, None, :]
        live_now = live_mask[:, position][:, None, None, None]
        memory = jnp.where(live_now, updated, memory)
        readings.append(jnp.einsum('shvk,shk->shv', memory, recept[:, position]))
    outputs_h = jnp.stack(readings, 1)
    head_mean = lax.optimization_barrier(jnp.mean(outputs_h, -1, keepdims=True))
    head_var = lax.optimization_barrier(jnp.mean(jnp.square(outputs_h - head_mean), -1, keepdims=True))
    normed = (outputs_h - head_mean) * lax.rsqrt(head_var + group_epsilon) * gain_vec.reshape(head_count, HEAD)
    mixed_out = normed * jax.nn.sigmoid(gate_pre) * live_mask[:, :, None, None].astype(jnp.float32)
    return (memory.reshape(state_in.shape), mixed_out.reshape(seq_count * NEW, head_count * HEAD).astype(jnp.bfloat16))

def reference(tokens, lengths, norm_gain, w_recept, w_keys, w_values, w_decay, w_rate, w_gate, decay_base, group_gain, w_out, states):
    current = tokens
    new_states = []
    for layer_id in range(2):
        wide_rows = current.astype(jnp.float32)
        inv_rms = lax.rsqrt(lax.optimization_barrier(jnp.sum(wide_rows * wide_rows, -1, keepdims=True)) / D + norm_epsilon)
        scaled = (wide_rows * norm_gain[layer_id]).astype(jnp.bfloat16)
        pieces = [(inv_rms * jnp.dot(scaled, matrix[layer_id], preferred_element_type=jnp.float32)).astype(jnp.bfloat16) for matrix in (w_recept, w_keys, w_values, w_decay, w_rate, w_gate)]
        memory, mixed_out = advance(states[layer_id], pieces, lengths, decay_base[layer_id], group_gain[layer_id])
        new_states.append(memory)
        current = (wide_rows + jnp.dot(mixed_out, w_out[layer_id], preferred_element_type=jnp.float32)).astype(jnp.bfloat16)
    return (current, jnp.stack(new_states))
```

```python
import functools

import jax
import jax.numpy as jnp
from jax import lax
from jax.experimental import pallas as pl
from jax.experimental.pallas import tpu as pltpu
from jax.sharding import PartitionSpec as P

HEAD = 64
NEW = 4
LANES = 128

norm_epsilon = 1e-06
unit_epsilon = 0.00064
group_epsilon = 0.00064

VMEM = pl.BlockSpec(memory_space=pltpu.VMEM)
SMEM = pl.BlockSpec(memory_space=pltpu.SMEM)


def iota(shape, dim):
    return lax.broadcasted_iota(jnp.int32, shape, dim)


def split_dot(x, ones):
    high = x.astype(jnp.bfloat16)
    low = (x - high.astype(jnp.float32)).astype(jnp.bfloat16)
    return jnp.dot(high, ones, preferred_element_type=jnp.float32) + jnp.dot(
        low, ones, preferred_element_type=jnp.float32
    )


def project_kernel(layer, rows, x_ref, gain_ref, *refs):
    *weight_refs, out_ref = refs
    owners, _, depth = x_ref.shape
    x = x_ref[...].reshape(owners * rows, depth).astype(jnp.float32)
    scaled = (x * gain_ref[layer : layer + 1, :]).astype(jnp.bfloat16)
    for first in range(0, 6, 2):
        pair = jnp.concatenate([weight_refs[first][layer], weight_refs[first + 1][layer]], 1)
        product = jnp.dot(scaled, pair, preferred_element_type=jnp.float32).astype(jnp.bfloat16)
        for half in range(2):
            out_ref[:, pl.ds((first + half) * rows, rows), :] = product[
                :, half * LANES : (half + 1) * LANES
            ].reshape(owners, rows, LANES)
    squares = jnp.sum(x * x, -1, keepdims=True)
    eye = iota((rows, LANES), 0) == iota((rows, LANES), 1)
    pick = iota((8, LANES), 0)
    for owner in range(owners):
        row = jnp.sum(
            jnp.where(eye, squares[owner * rows : (owner + 1) * rows], 0.0), 0, keepdims=True
        )
        high = row.astype(jnp.bfloat16).astype(jnp.float32)
        tail = jnp.where(pick == 0, high, jnp.where(pick == 1, row - high, 0.0))
        out_ref[owner, pl.ds(6 * rows, 8), :] = tail.astype(jnp.bfloat16)


def advance_kernel(layer, rows, width, arrived_ref, lengths_ref, base_ref, gain_ref, state_ref, *refs):
    mixed_ref, new_ref, line_ref, read_ref = refs[-4:]
    seqs = rows // NEW
    total = jnp.sum(arrived_ref[...].astype(jnp.float32), 0)
    eye = iota((rows, LANES), 0) == iota((rows, LANES), 1)
    square = total[6 * rows : 6 * rows + 1] + total[6 * rows + 1 : 6 * rows + 2]
    square = jnp.sum(jnp.where(eye, square, 0.0), 1, keepdims=True)
    inv_rms = lax.rsqrt(square / width + norm_epsilon)
    recept, keys, values, decay_pre, rate_pre, gate_pre = [
        (inv_rms * total[role * rows : (role + 1) * rows]).astype(jnp.bfloat16).astype(jnp.float32)
        for role in range(6)
    ]
    same_head = (iota((LANES, LANES), 0) // HEAD == iota((LANES, LANES), 1) // HEAD).astype(
        jnp.float32
    ).astype(jnp.bfloat16)
    log_rate = base_ref[layer : layer + 1, :] + decay_pre
    decays = jnp.exp(jax.nn.sigmoid(log_rate) * (-0.6065306597126334))
    rates = jax.nn.sigmoid(rate_pre)
    unit = keys * lax.rsqrt(split_dot(keys * keys, same_head) + unit_epsilon)
    slot = iota((rows, LANES), 0)
    limit = jnp.zeros((rows, LANES), jnp.int32)
    for seq in range(seqs):
        limit = jnp.where(slot // NEW == seq, lengths_ref[seq], limit)
    live = slot % NEW < limit
    decays = jnp.where(live, decays, 1.0)
    unit = jnp.where(live, unit, 0.0)
    keys = jnp.where(live, keys, 0.0)
    lane = iota((rows, LANES), 1)
    for place, line in enumerate((decays, unit, unit * rates, keys, recept)):
        turned = pltpu.roll(line, HEAD, 1)
        line_ref[2 * place] = jnp.where(lane < HEAD, line, turned)
        line_ref[2 * place + 1] = jnp.where(lane < HEAD, turned, line)
    line_ref[10] = values
    even = iota((8, LANES), 0) % 2 == 0
    block_row, block_lane = iota((HEAD, LANES), 0), iota((HEAD, LANES), 1)
    place_mask = (block_row % 2 == block_lane // HEAD) & (block_row // 2 == block_lane % HEAD // 2)
    parity = (iota((LANES, LANES), 0) % 2 == iota((LANES, LANES), 1) // HEAD).astype(
        jnp.float32
    ).astype(jnp.bfloat16)
    parity_back = (iota((LANES, LANES), 1) % 2 == iota((LANES, LANES), 0) // HEAD).astype(
        jnp.float32
    ).astype(jnp.bfloat16)

    def spread(place, token):
        return jnp.where(
            even, line_ref[2 * place, pl.ds(token, 1), :], line_ref[2 * place + 1, pl.ds(token, 1), :]
        )[None]

    state = [
        state_ref[pl.ds(seq * HEAD, HEAD), :].reshape(8, 8, LANES) for seq in range(seqs)
    ]
    for position in range(NEW):
        tokens = [seq * NEW + position for seq in range(seqs)]
        against = jnp.concatenate(
            [(s * spread(1, t)).reshape(HEAD, LANES) for s, t in zip(state, tokens)], 0
        )
        removed = split_dot(against, same_head)
        written = jnp.concatenate(
            [jnp.where(place_mask, line_ref[10, pl.ds(t, 1), :], 0.0) for t in tokens], 0
        ).astype(jnp.bfloat16)
        written = jnp.dot(written, parity, preferred_element_type=jnp.float32)
        for seq, t in enumerate(tokens):
            part = slice(seq * HEAD, (seq + 1) * HEAD)
            state[seq] = (
                state[seq] * spread(0, t)
                - removed[part].reshape(8, 8, LANES) * spread(2, t)
                + written[part].reshape(8, 8, LANES) * spread(3, t)
            )
        read = jnp.concatenate(
            [(s * spread(4, t)).reshape(HEAD, LANES) for s, t in zip(state, tokens)], 0
        )
        read = split_dot(read, parity_back)
        for seq, t in enumerate(tokens):
            part = slice(seq * HEAD, (seq + 1) * HEAD)
            read_ref[pl.ds(t, 1), :] = jnp.sum(
                jnp.where(place_mask, read[part], 0.0), 0, keepdims=True
            )
    for seq in range(seqs):
        new_ref[0, pl.ds(seq * HEAD, HEAD), :] = state[seq].reshape(HEAD, LANES)
    read = read_ref[...]
    centred = read - split_dot(read, same_head) / HEAD
    variance = split_dot(centred * centred, same_head) / HEAD
    normed = centred * lax.rsqrt(variance + group_epsilon) * gain_ref[layer : layer + 1, :]
    mixed_ref[...] = jnp.where(live, normed * jax.nn.sigmoid(gate_pre), 0.0).astype(jnp.bfloat16)


def project(layer, x, gain, weights):
    owners, rows, _ = x.shape
    return pl.pallas_call(
        functools.partial(project_kernel, layer, rows),
        out_shape=jax.ShapeDtypeStruct((owners, 6 * rows + 8, LANES), jnp.bfloat16),
        in_specs=[VMEM] * 8,
        out_specs=VMEM,
        compiler_params=pltpu.CompilerParams(vmem_limit_bytes=24 * 2**20),
        cost_estimate=pl.CostEstimate(flops=2 * 10**8, bytes_accessed=2 * 10**6, transcendentals=0),
    )(x, gain, *weights)


def advance(layer, width, arrived, lengths, base, gain, states, held):
    rows = lengths.shape[0] * NEW
    state_rows = states.shape[1]
    block = pl.BlockSpec((1, state_rows, LANES), lambda i: (layer, 0, 0))
    in_block = pl.BlockSpec((None, state_rows, LANES), lambda i: (layer, 0, 0))
    operands = [arrived, lengths, base, gain, states]
    in_specs = [VMEM, SMEM, VMEM, VMEM, in_block]
    aliases = {}
    if held is not None:
        aliases = {len(operands): 1}
        operands.append(held)
        in_specs.append(pl.BlockSpec(memory_space=pl.ANY))
    return pl.pallas_call(
        functools.partial(advance_kernel, layer, rows, width),
        grid=(1,),
        out_shape=(
            jax.ShapeDtypeStruct((rows, LANES), jnp.bfloat16),
            jax.ShapeDtypeStruct(states.shape, jnp.float32),
        ),
        in_specs=in_specs,
        out_specs=(pl.BlockSpec((rows, LANES), lambda i: (0, 0)), block),
        scratch_shapes=[
            pltpu.VMEM((11, rows, LANES), jnp.float32),
            pltpu.VMEM((rows, LANES), jnp.float32),
        ],
        input_output_aliases=aliases,
        compiler_params=pltpu.CompilerParams(vmem_limit_bytes=24 * 2**20),
        cost_estimate=pl.CostEstimate(flops=2 * 10**8, bytes_accessed=2 * 10**6, transcendentals=0),
    )(*operands)


def gather_blocks(x, axis):
    copies = jnp.broadcast_to(x, (lax.axis_size(axis), *x.shape))
    return lax.all_to_all(copies, axis, split_axis=0, concat_axis=0, tiled=True)


def per_device(
    tokens,
    lengths,
    norm_gain,
    w_recept,
    w_keys,
    w_values,
    w_decay,
    w_rate,
    w_gate,
    decay_base,
    group_gain,
    w_out,
    states,
):
    weights = (w_recept, w_keys, w_values, w_decay, w_rate, w_gate)
    own_count, depth = tokens.shape
    width = depth * lax.axis_size("dp")
    blocks, seqs, heads, _ = states.shape
    folded = states.reshape(blocks, seqs, heads, HEAD // 2, LANES)
    folded = jnp.swapaxes(folded, 2, 3).reshape(blocks, seqs * HEAD, LANES)
    own_rows = tokens
    held = None
    for layer in range(2):
        gathered = gather_blocks(own_rows, "tp")
        partial_sums = project(layer, gathered, norm_gain, weights)
        arrived = lax.all_to_all(partial_sums, "dp", 0, 0, tiled=True)
        mixed, held = advance(
            layer, width, arrived, lengths, decay_base, group_gain, folded, held
        )
        everyone = gather_blocks(mixed, "dp")
        product = jnp.dot(
            everyone.reshape(-1, LANES), w_out[layer], preferred_element_type=jnp.float32
        )
        product = product.astype(jnp.bfloat16).reshape(-1, own_count, depth)
        summed = lax.all_to_all(product, "tp", 0, 0, tiled=True)
        own_rows = (
            own_rows.astype(jnp.float32) + jnp.sum(summed.astype(jnp.float32), 0)
        ).astype(jnp.bfloat16)
    new_states = jnp.swapaxes(held.reshape(blocks, seqs, HEAD // 2, heads, LANES), 2, 3)
    return (own_rows, new_states.reshape(states.shape))


def solution(mesh):
    placed = (
        P(("grp", "tp"), "dp"),
        P(("grp", "dp")),
        P(None, "dp"),
        P(None, "dp", "tp"),
        P(None, "dp", "tp"),
        P(None, "dp", "tp"),
        P(None, "dp", "tp"),
        P(None, "dp", "tp"),
        P(None, "dp", "tp"),
        P(None, "tp"),
        P(None, "tp"),
        P(None, "tp", "dp"),
        P(None, ("grp", "dp"), "tp", None),
    )
    return jax.shard_map(
        per_device,
        mesh=mesh,
        in_specs=placed,
        out_specs=(P(("grp", "tp"), "dp"), P(None, ("grp", "dp"), "tp", None)),
        check_vma=False,
    )
```

```python
import functools

import jax
import jax.numpy as jnp
from jax import lax
from jax.experimental import pallas as pl
from jax.experimental.pallas import tpu as pltpu
from jax.sharding import PartitionSpec as P

HEAD = 64
NEW = 4
LANES = 128

norm_epsilon = 1e-06
unit_epsilon = 0.00064
group_epsilon = 0.00064

VMEM = pl.BlockSpec(memory_space=pltpu.VMEM)
SMEM = pl.BlockSpec(memory_space=pltpu.SMEM)


def iota(shape, dim):
    return lax.broadcasted_iota(jnp.int32, shape, dim)


def split_dot(x, ones):
    high = x.astype(jnp.bfloat16)
    low = (x - high.astype(jnp.float32)).astype(jnp.bfloat16)
    return jnp.dot(high, ones, preferred_element_type=jnp.float32) + jnp.dot(
        low, ones, preferred_element_type=jnp.float32
    )


def project_kernel(layer, far, groups, place_ref, x_ref, gain_ref, *refs):
    out_ref = refs[-1]
    core, column = place_ref[0], place_ref[1]
    blocks, rows, depth = x_ref.shape
    half = rows // 2
    first_half = core == (1 if far else 0)
    x = x_ref[...].astype(jnp.float32)
    x = jnp.where(first_half, x[:, :half], x[:, half:]).reshape(blocks * half, depth)
    scaled = (x * gain_ref[layer : layer + 1, :]).astype(jnp.bfloat16)
    squares = jnp.sum(x * x, -1, keepdims=True)
    eye = iota((half, LANES), 0) == iota((half, LANES), 1)
    pick = iota((8, LANES), 0)
    for group in range(groups):
        owner = jnp.bitwise_xor(column, group) if groups > 1 else 0
        for first in range(0, 6, 2):
            if group:
                pair = [refs[6][first], refs[6][first + 1]]
            else:
                pair = [refs[first][layer], refs[first + 1][layer]]
            product = jnp.dot(
                scaled, jnp.concatenate(pair, 1), preferred_element_type=jnp.float32
            )
            for side in range(2):
                part = product[:, side * LANES : (side + 1) * LANES].reshape(blocks, half, LANES)
                where = pl.ds((first + side) * half, half)
                if not far:
                    part = part + refs[-2][owner, :, where, :].astype(jnp.float32)
                out_ref[owner, :, where, :] = part.astype(jnp.bfloat16)
        for block in range(blocks):
            row = jnp.sum(
                jnp.where(eye, squares[block * half : (block + 1) * half], 0.0), 0, keepdims=True
            )
            if not far:
                came = refs[-2][owner, block, pl.ds(6 * half, 8), :].astype(jnp.float32)
                row = row + came[0:1] + came[1:2]
            high = row.astype(jnp.bfloat16).astype(jnp.float32)
            tail = jnp.where(pick == 0, high, jnp.where(pick == 1, row - high, 0.0))
            out_ref[owner, block, pl.ds(6 * half, 8), :] = tail.astype(jnp.bfloat16)


def advance_kernel(layer, rows, width, arrived_ref, lengths_ref, base_ref, gain_ref, state_ref, *refs):
    mixed_ref, new_ref, line_ref, read_ref = refs[-4:]
    seqs = rows // NEW
    parts, part_rows = arrived_ref.shape[0], (arrived_ref.shape[1] - 8) // 6
    eye = iota((part_rows, LANES), 0) == iota((part_rows, LANES), 1)
    scaled = []
    for part in range(rows // part_rows):
        outer, core = part // 2, part % 2
        chips = parts * part_rows // rows
        total = arrived_ref[outer * chips * 2 + core].astype(jnp.float32)
        for chip in range(1, chips):
            total += arrived_ref[(outer * chips + chip) * 2 + core].astype(jnp.float32)
        square = total[6 * part_rows : 6 * part_rows + 1] + total[6 * part_rows + 1 : 6 * part_rows + 2]
        square = jnp.sum(jnp.where(eye, square, 0.0), 1, keepdims=True)
        inv_rms = lax.rsqrt(square / width + norm_epsilon)
        scaled.append(
            [inv_rms * total[role * part_rows : (role + 1) * part_rows] for role in range(6)]
        )
    recept, keys, values, decay_pre, rate_pre, gate_pre = [
        jnp.concatenate([part[role] for part in scaled], 0).astype(jnp.bfloat16).astype(jnp.float32)
        for role in range(6)
    ]
    same_head = (iota((LANES, LANES), 0) // HEAD == iota((LANES, LANES), 1) // HEAD).astype(
        jnp.float32
    ).astype(jnp.bfloat16)
    log_rate = base_ref[layer : layer + 1, :] + decay_pre
    decays = jnp.exp(jax.nn.sigmoid(log_rate) * (-0.6065306597126334))
    rates = jax.nn.sigmoid(rate_pre)
    unit = keys * lax.rsqrt(split_dot(keys * keys, same_head) + unit_epsilon)
    slot = iota((rows, LANES), 0)
    limit = jnp.zeros((rows, LANES), jnp.int32)
    for seq in range(seqs):
        limit = jnp.where(slot // NEW == seq, lengths_ref[seq], limit)
    live = slot % NEW < limit
    decays = jnp.where(live, decays, 1.0)
    unit = jnp.where(live, unit, 0.0)
    keys = jnp.where(live, keys, 0.0)
    lane = iota((rows, LANES), 1)
    for place, line in enumerate((decays, unit, unit * rates, keys, recept)):
        turned = pltpu.roll(line, HEAD, 1)
        line_ref[2 * place] = jnp.where(lane < HEAD, line, turned)
        line_ref[2 * place + 1] = jnp.where(lane < HEAD, turned, line)
    line_ref[10] = values
    even = iota((8, LANES), 0) % 2 == 0
    block_row, block_lane = iota((HEAD, LANES), 0), iota((HEAD, LANES), 1)
    place_mask = (block_row % 2 == block_lane // HEAD) & (block_row // 2 == block_lane % HEAD // 2)
    parity = (iota((LANES, LANES), 0) % 2 == iota((LANES, LANES), 1) // HEAD).astype(
        jnp.float32
    ).astype(jnp.bfloat16)
    parity_back = (iota((LANES, LANES), 1) % 2 == iota((LANES, LANES), 0) // HEAD).astype(
        jnp.float32
    ).astype(jnp.bfloat16)

    def spread(place, token):
        return jnp.where(
            even, line_ref[2 * place, pl.ds(token, 1), :], line_ref[2 * place + 1, pl.ds(token, 1), :]
        )[None]

    state = [
        state_ref[pl.ds(seq * HEAD, HEAD), :].reshape(8, 8, LANES) for seq in range(seqs)
    ]
    for position in range(NEW):
        tokens = [seq * NEW + position for seq in range(seqs)]
        against = jnp.concatenate(
            [(s * spread(1, t)).reshape(HEAD, LANES) for s, t in zip(state, tokens)], 0
        )
        removed = split_dot(against, same_head)
        written = jnp.concatenate(
            [jnp.where(place_mask, line_ref[10, pl.ds(t, 1), :], 0.0) for t in tokens], 0
        ).astype(jnp.bfloat16)
        written = jnp.dot(written, parity, preferred_element_type=jnp.float32)
        for seq, t in enumerate(tokens):
            part = slice(seq * HEAD, (seq + 1) * HEAD)
            state[seq] = (
                state[seq] * spread(0, t)
                - removed[part].reshape(8, 8, LANES) * spread(2, t)
                + written[part].reshape(8, 8, LANES) * spread(3, t)
            )
        read = jnp.concatenate(
            [(s * spread(4, t)).reshape(HEAD, LANES) for s, t in zip(state, tokens)], 0
        )
        read = split_dot(read, parity_back)
        for seq, t in enumerate(tokens):
            part = slice(seq * HEAD, (seq + 1) * HEAD)
            read_ref[pl.ds(t, 1), :] = jnp.sum(
                jnp.where(place_mask, read[part], 0.0), 0, keepdims=True
            )
    for seq in range(seqs):
        new_ref[0, pl.ds(seq * HEAD, HEAD), :] = state[seq].reshape(HEAD, LANES)
    read = read_ref[...]
    centred = read - split_dot(read, same_head) / HEAD
    variance = split_dot(centred * centred, same_head) / HEAD
    normed = centred * lax.rsqrt(variance + group_epsilon) * gain_ref[layer : layer + 1, :]
    mixed_ref[...] = jnp.where(live, normed * jax.nn.sigmoid(gate_pre), 0.0).astype(jnp.bfloat16)


def out_kernel(layer, place_ref, mixed_ref, own_ref, other_ref, out_ref):
    pair, blocks, rows, _ = mixed_ref.shape
    first = place_ref[1] == 0
    own, other = own_ref[layer], other_ref[layer]
    total = 0.0
    for member, matrix in enumerate(
        (jnp.where(first, own, other), jnp.where(first, other, own))
    ):
        total += jnp.dot(
            mixed_ref[member].reshape(blocks * rows, LANES),
            matrix,
            preferred_element_type=jnp.float32,
        )
    out_ref[...] = total.astype(jnp.bfloat16).reshape(out_ref.shape)


def params():
    return {
        "compiler_params": pltpu.CompilerParams(vmem_limit_bytes=24 * 2**20),
        "cost_estimate": pl.CostEstimate(
            flops=10**8, bytes_accessed=2 * 10**6, transcendentals=0
        ),
    }


def project(layer, far, place, x, gain, weights, others, came):
    blocks, rows, _ = x.shape
    groups = 1 if others is None else 2
    extra = ([] if others is None else [others]) + ([] if came is None else [came])
    return pl.pallas_call(
        functools.partial(project_kernel, layer, far, groups),
        out_shape=jax.ShapeDtypeStruct((groups, blocks, 3 * rows + 8, LANES), jnp.bfloat16),
        in_specs=[SMEM] + [VMEM] * (8 + len(extra)),
        out_specs=VMEM,
        **params(),
    )(place, x, gain, *weights, *extra)


def project_out(layer, place, mixed, own, other):
    _, blocks, rows, _ = mixed.shape
    return pl.pallas_call(
        functools.partial(out_kernel, layer),
        out_shape=jax.ShapeDtypeStruct((blocks, rows, own.shape[2]), jnp.bfloat16),
        in_specs=[SMEM] + [VMEM] * 3,
        out_specs=VMEM,
        **params(),
    )(place, mixed, own, other)


def advance(layer, width, arrived, lengths, base, gain, states, held, awaited):
    rows = lengths.shape[0] * NEW
    state_rows = states.shape[1]
    block = pl.BlockSpec((1, state_rows, LANES), lambda i: (layer, 0, 0))
    in_block = pl.BlockSpec((None, state_rows, LANES), lambda i: (layer, 0, 0))
    operands = [arrived, lengths, base, gain, states]
    in_specs = [VMEM, SMEM, VMEM, VMEM, in_block]
    aliases = {}
    if held is not None:
        aliases = {len(operands): 1}
        operands.append(held)
        in_specs.append(pl.BlockSpec(memory_space=pl.ANY))
    operands.extend(awaited)
    in_specs.extend([pl.BlockSpec(memory_space=pl.ANY)] * len(awaited))
    return pl.pallas_call(
        functools.partial(advance_kernel, layer, rows, width),
        grid=(1,),
        out_shape=(
            jax.ShapeDtypeStruct((rows, LANES), jnp.bfloat16),
            jax.ShapeDtypeStruct(states.shape, jnp.float32),
        ),
        in_specs=in_specs,
        out_specs=(pl.BlockSpec((rows, LANES), lambda i: (0, 0)), block),
        scratch_shapes=[
            pltpu.VMEM((11, rows, LANES), jnp.float32),
            pltpu.VMEM((rows, LANES), jnp.float32),
        ],
        input_output_aliases=aliases,
        **params(),
    )(*operands)


def exchange(x, axis, groups=None):
    return lax.all_to_all(x, axis, 0, 0, tiled=True, axis_index_groups=groups)


def from_partner(x, axis):
    return lax.ppermute(x, axis, [(i, i ^ 1) for i in range(lax.axis_size(axis))])


def per_device(
    tokens,
    lengths,
    norm_gain,
    w_recept,
    w_keys,
    w_values,
    w_decay,
    w_rate,
    w_gate,
    decay_base,
    group_gain,
    w_out,
    states,
):
    weights = (w_recept, w_keys, w_values, w_decay, w_rate, w_gate)
    own_count, depth = tokens.shape
    width = depth * lax.axis_size("dp")
    blocks, seqs, heads, _ = states.shape
    folded = states.reshape(blocks, seqs, heads, HEAD // 2, LANES)
    folded = jnp.swapaxes(folded, 2, 3).reshape(blocks, seqs * HEAD, LANES)
    columns, owners = lax.axis_size("tp"), lax.axis_size("dp")
    place = jnp.stack([lax.axis_index("dp") % 2, lax.axis_index("tp") % 2])
    both = ("tp", "dp")
    pairs = [
        [column * owners + owner for column in (first, first + 1) for owner in range(owners)]
        for first in range(0, columns, 2)
    ]
    half = own_count // 2
    other_out = from_partner(w_out, "tp")
    other_weights = from_partner(jnp.stack([weight[1] for weight in weights]), "tp")
    own_rows = tokens
    held = None
    for layer in range(2):
        if layer == 0:
            spread = jnp.broadcast_to(own_rows, (columns, own_count, depth))
            others = None
        else:
            spread = jnp.broadcast_to(
                own_rows.reshape(2, half, depth), (columns // 2, 2, half, depth)
            ).reshape(columns, half, depth)
            others = other_weights
        gathered = exchange(spread, "tp")
        far = project(layer, True, place, gathered, norm_gain, weights, others, None)
        came = from_partner(far, "dp")
        near = project(layer, False, place, gathered, norm_gain, weights, others, came)
        near = near.reshape(-1, *near.shape[2:])
        arrived = exchange(near, "dp") if layer == 0 else exchange(near, both, pairs)
        mixed, held = advance(
            layer, width, arrived, lengths, decay_base, group_gain, folded, held,
            [] if layer else [other_out, other_weights],
        )
        shared = jnp.broadcast_to(mixed.reshape(2, 1, half, LANES), (2, owners, half, LANES))
        shared = exchange(shared.reshape(2 * owners, half, LANES), both, pairs)
        product = project_out(
            layer, place, shared.reshape(2, owners, half, LANES), w_out, other_out
        )
        summed = exchange(product, "tp").astype(jnp.float32)
        summed = jnp.sum(summed.reshape(columns // 2, 2, half, depth), 0)
        own_rows = (
            own_rows.astype(jnp.float32) + summed.reshape(own_count, depth)
        ).astype(jnp.bfloat16)
    new_states = jnp.swapaxes(held.reshape(blocks, seqs, HEAD // 2, heads, LANES), 2, 3)
    return (own_rows, new_states.reshape(states.shape))


def solution(mesh):
    placed = (
        P(("grp", "tp"), "dp"),
        P(("grp", "dp")),
        P(None, "dp"),
        P(None, "dp", "tp"),
        P(None, "dp", "tp"),
        P(None, "dp", "tp"),
        P(None, "dp", "tp"),
        P(None, "dp", "tp"),
        P(None, "dp", "tp"),
        P(None, "tp"),
        P(None, "tp"),
        P(None, "tp", "dp"),
        P(None, ("grp", "dp"), "tp", None),
    )
    return jax.shard_map(
        per_device,
        mesh=mesh,
        in_specs=placed,
        out_specs=(P(("grp", "tp"), "dp"), P(None, ("grp", "dp"), "tp", None)),
        check_vma=False,
    )
```

```python
import functools

import jax
import jax.numpy as jnp
from jax import lax
from jax.experimental import pallas as pl
from jax.experimental.pallas import tpu as pltpu
from jax.sharding import PartitionSpec as P


HEAD = 64
NEW = 4
LANES = 128

norm_epsilon = 1e-06
unit_epsilon = 0.00064
group_epsilon = 0.00064

VMEM = pl.BlockSpec(memory_space=pltpu.VMEM)
SMEM = pl.BlockSpec(memory_space=pltpu.SMEM)


def iota(shape, dim):
    return lax.broadcasted_iota(jnp.int32, shape, dim)


def split_dot(x, ones):
    high = x.astype(jnp.bfloat16)
    low = (x - high.astype(jnp.float32)).astype(jnp.bfloat16)
    return jnp.dot(high, ones, preferred_element_type=jnp.float32) + jnp.dot(
        low, ones, preferred_element_type=jnp.float32
    )


def project_kernel(layer, far, groups, place_ref, x_ref, gain_ref, *refs):
    out_ref = refs[-1]
    core, column = place_ref[0], place_ref[1]
    blocks, rows, depth = x_ref.shape
    half = rows // 2
    first_half = core == (1 if far else 0)
    x = x_ref[...].astype(jnp.float32)
    x = jnp.where(first_half, x[:, :half], x[:, half:]).reshape(blocks * half, depth)
    scaled = (x * gain_ref[layer : layer + 1, :]).astype(jnp.bfloat16)
    squares = jnp.sum(x * x, -1, keepdims=True)
    eye = iota((half, LANES), 0) == iota((half, LANES), 1)
    pick = iota((8, LANES), 0)
    for group in range(groups):
        owner = jnp.bitwise_xor(column, group) if groups > 1 else 0
        for first in range(0, 6, 2):
            if group:
                pair = [refs[6][first], refs[6][first + 1]]
            else:
                pair = [refs[first][layer], refs[first + 1][layer]]
            product = jnp.dot(
                scaled, jnp.concatenate(pair, 1), preferred_element_type=jnp.float32
            )
            for side in range(2):
                part = product[:, side * LANES : (side + 1) * LANES].reshape(blocks, half, LANES)
                where = pl.ds((first + side) * half, half)
                if not far:
                    part = part + refs[-2][owner, :, where, :].astype(jnp.float32)
                out_ref[owner, :, where, :] = part.astype(jnp.bfloat16)
        for block in range(blocks):
            row = jnp.sum(
                jnp.where(eye, squares[block * half : (block + 1) * half], 0.0), 0, keepdims=True
            )
            if not far:
                came = refs[-2][owner, block, pl.ds(6 * half, 8), :].astype(jnp.float32)
                row = row + came[0:1] + came[1:2]
            high = row.astype(jnp.bfloat16).astype(jnp.float32)
            tail = jnp.where(pick == 0, high, jnp.where(pick == 1, row - high, 0.0))
            out_ref[owner, block, pl.ds(6 * half, 8), :] = tail.astype(jnp.bfloat16)


def advance_kernel(layer, rows, width, arrived_ref, lengths_ref, base_ref, gain_ref, state_ref, *refs):
    mixed_ref, new_ref, line_ref, read_ref = refs[-4:]
    seqs = rows // NEW
    parts, part_rows = arrived_ref.shape[0], (arrived_ref.shape[1] - 8) // 6
    eye = iota((part_rows, LANES), 0) == iota((part_rows, LANES), 1)
    scaled = []
    for part in range(rows // part_rows):
        outer, core = part // 2, part % 2
        chips = parts * part_rows // rows
        total = arrived_ref[outer * chips * 2 + core].astype(jnp.float32)
        for chip in range(1, chips):
            total += arrived_ref[(outer * chips + chip) * 2 + core].astype(jnp.float32)
        square = total[6 * part_rows : 6 * part_rows + 1] + total[6 * part_rows + 1 : 6 * part_rows + 2]
        square = jnp.sum(jnp.where(eye, square, 0.0), 1, keepdims=True)
        inv_rms = lax.rsqrt(square / width + norm_epsilon)
        scaled.append(
            [inv_rms * total[role * part_rows : (role + 1) * part_rows] for role in range(6)]
        )
    recept, keys, values, decay_pre, rate_pre, gate_pre = [
        jnp.concatenate([part[role] for part in scaled], 0).astype(jnp.bfloat16).astype(jnp.float32)
        for role in range(6)
    ]
    same_head = (iota((LANES, LANES), 0) // HEAD == iota((LANES, LANES), 1) // HEAD).astype(
        jnp.float32
    ).astype(jnp.bfloat16)
    log_rate = base_ref[layer : layer + 1, :] + decay_pre
    decays = jnp.exp(jax.nn.sigmoid(log_rate) * (-0.6065306597126334))
    rates = jax.nn.sigmoid(rate_pre)
    unit = keys * lax.rsqrt(split_dot(keys * keys, same_head) + unit_epsilon)
    slot = iota((rows, LANES), 0)
    limit = jnp.zeros((rows, LANES), jnp.int32)
    for seq in range(seqs):
        limit = jnp.where(slot // NEW == seq, lengths_ref[seq], limit)
    live = slot % NEW < limit
    decays = jnp.where(live, decays, 1.0)
    unit = jnp.where(live, unit, 0.0)
    keys = jnp.where(live, keys, 0.0)
    lane = iota((rows, LANES), 1)
    for place, line in enumerate((decays, unit, unit * rates, keys, recept)):
        turned = pltpu.roll(line, HEAD, 1)
        line_ref[2 * place] = jnp.where(lane < HEAD, line, turned)
        line_ref[2 * place + 1] = jnp.where(lane < HEAD, turned, line)
    line_ref[10] = values
    even = iota((8, LANES), 0) % 2 == 0
    block_row, block_lane = iota((HEAD, LANES), 0), iota((HEAD, LANES), 1)
    place_mask = (block_row % 2 == block_lane // HEAD) & (block_row // 2 == block_lane % HEAD // 2)
    parity = (iota((LANES, LANES), 0) % 2 == iota((LANES, LANES), 1) // HEAD).astype(
        jnp.float32
    ).astype(jnp.bfloat16)
    parity_back = (iota((LANES, LANES), 1) % 2 == iota((LANES, LANES), 0) // HEAD).astype(
        jnp.float32
    ).astype(jnp.bfloat16)

    def spread(place, token):
        return jnp.where(
            even, line_ref[2 * place, pl.ds(token, 1), :], line_ref[2 * place + 1, pl.ds(token, 1), :]
        )[None]

    state = [
        state_ref[pl.ds(seq * HEAD, HEAD), :].reshape(8, 8, LANES) for seq in range(seqs)
    ]
    for position in range(NEW):
        tokens = [seq * NEW + position for seq in range(seqs)]
        against = jnp.concatenate(
            [(s * spread(1, t)).reshape(HEAD, LANES) for s, t in zip(state, tokens)], 0
        )
        removed = split_dot(against, same_head)
        written = jnp.concatenate(
            [jnp.where(place_mask, line_ref[10, pl.ds(t, 1), :], 0.0) for t in tokens], 0
        ).astype(jnp.bfloat16)
        written = jnp.dot(written, parity, preferred_element_type=jnp.float32)
        for seq, t in enumerate(tokens):
            part = slice(seq * HEAD, (seq + 1) * HEAD)
            state[seq] = (
                state[seq] * spread(0, t)
                - removed[part].reshape(8, 8, LANES) * spread(2, t)
                + written[part].reshape(8, 8, LANES) * spread(3, t)
            )
        read = jnp.concatenate(
            [(s * spread(4, t)).reshape(HEAD, LANES) for s, t in zip(state, tokens)], 0
        )
        read = split_dot(read, parity_back)
        for seq, t in enumerate(tokens):
            part = slice(seq * HEAD, (seq + 1) * HEAD)
            read_ref[pl.ds(t, 1), :] = jnp.sum(
                jnp.where(place_mask, read[part], 0.0), 0, keepdims=True
            )
    for seq in range(seqs):
        new_ref[0, pl.ds(seq * HEAD, HEAD), :] = state[seq].reshape(HEAD, LANES)
    read = read_ref[...]
    centred = read - split_dot(read, same_head) / HEAD
    variance = split_dot(centred * centred, same_head) / HEAD
    normed = centred * lax.rsqrt(variance + group_epsilon) * gain_ref[layer : layer + 1, :]
    mixed_ref[...] = jnp.where(live, normed * jax.nn.sigmoid(gate_pre), 0.0).astype(jnp.bfloat16)


def out_kernel(layer, place_ref, mixed_ref, own_ref, other_ref, *refs):
    out_ref = refs[-1]
    _, blocks, rows, _ = mixed_ref.shape
    first = place_ref[1] == 0
    own, other = own_ref[layer], other_ref[layer]
    total = 0.0
    for member, matrix in enumerate(
        (jnp.where(first, own, other), jnp.where(first, other, own))
    ):
        total += jnp.dot(
            mixed_ref[member].reshape(blocks * rows, LANES),
            matrix,
            preferred_element_type=jnp.float32,
        )
    out_ref[...] = total.astype(jnp.bfloat16).reshape(out_ref.shape)


def params():
    return {
        "compiler_params": pltpu.CompilerParams(vmem_limit_bytes=24 * 2**20),
        "cost_estimate": pl.CostEstimate(
            flops=10**8, bytes_accessed=2 * 10**6, transcendentals=0
        ),
    }


def project(layer, far, place, x, gain, weights, others, came):
    blocks, rows, _ = x.shape
    groups = 1 if others is None else 2
    extra = ([] if others is None else [others]) + ([] if came is None else [came])
    return pl.pallas_call(
        functools.partial(project_kernel, layer, far, groups),
        out_shape=jax.ShapeDtypeStruct((groups, blocks, 3 * rows + 8, LANES), jnp.bfloat16),
        in_specs=[SMEM] + [VMEM] * (8 + len(extra)),
        out_specs=VMEM,
        **params(),
    )(place, x, gain, *weights, *extra)


def project_out(layer, place, mixed, own, other, awaited):
    _, blocks, rows, _ = mixed.shape
    return pl.pallas_call(
        functools.partial(out_kernel, layer),
        out_shape=jax.ShapeDtypeStruct((blocks, rows, own.shape[2]), jnp.bfloat16),
        in_specs=[SMEM] + [VMEM] * 3 + [pl.BlockSpec(memory_space=pl.ANY)] * len(awaited),
        out_specs=VMEM,
        **params(),
    )(place, mixed, own, other, *awaited)


def advance(layer, width, arrived, lengths, base, gain, states, held, awaited):
    rows = lengths.shape[0] * NEW
    state_rows = states.shape[1]
    block = pl.BlockSpec((1, state_rows, LANES), lambda i: (layer, 0, 0))
    in_block = pl.BlockSpec((None, state_rows, LANES), lambda i: (layer, 0, 0))
    operands = [arrived, lengths, base, gain, states]
    in_specs = [VMEM, SMEM, VMEM, VMEM, in_block]
    aliases = {}
    if held is not None:
        aliases = {len(operands): 1}
        operands.append(held)
        in_specs.append(pl.BlockSpec(memory_space=pl.ANY))
    operands.extend(awaited)
    in_specs.extend([pl.BlockSpec(memory_space=pl.ANY)] * len(awaited))
    return pl.pallas_call(
        functools.partial(advance_kernel, layer, rows, width),
        grid=(1,),
        out_shape=(
            jax.ShapeDtypeStruct((rows, LANES), jnp.bfloat16),
            jax.ShapeDtypeStruct(states.shape, jnp.float32),
        ),
        in_specs=in_specs,
        out_specs=(pl.BlockSpec((rows, LANES), lambda i: (0, 0)), block),
        scratch_shapes=[
            pltpu.VMEM((11, rows, LANES), jnp.float32),
            pltpu.VMEM((rows, LANES), jnp.float32),
        ],
        input_output_aliases=aliases,
        **params(),
    )(*operands)


def exchange(x, axis, groups=None):
    return lax.all_to_all(x, axis, 0, 0, tiled=True, axis_index_groups=groups)


def from_partner(x, axis):
    return lax.ppermute(x, axis, [(i, i ^ 1) for i in range(lax.axis_size(axis))])


def per_device(
    tokens,
    lengths,
    norm_gain,
    w_recept,
    w_keys,
    w_values,
    w_decay,
    w_rate,
    w_gate,
    decay_base,
    group_gain,
    w_out,
    states,
):
    weights = (w_recept, w_keys, w_values, w_decay, w_rate, w_gate)
    own_count, depth = tokens.shape
    width = depth * lax.axis_size("dp")
    blocks, seqs, heads, _ = states.shape
    folded = states.reshape(blocks, seqs, heads, HEAD // 2, LANES)
    folded = jnp.swapaxes(folded, 2, 3).reshape(blocks, seqs * HEAD, LANES)
    columns, owners = lax.axis_size("tp"), lax.axis_size("dp")
    place = jnp.stack([lax.axis_index("dp") % 2, lax.axis_index("tp") % 2])
    both = ("tp", "dp")
    pairs = [
        [column * owners + owner for column in (first, first + 1) for owner in range(owners)]
        for first in range(0, columns, 2)
    ]
    half = own_count // 2
    other_out = from_partner(w_out, "tp")
    other_weights = from_partner(jnp.stack([weight[1] for weight in weights]), "tp")
    own_rows = tokens
    held = None
    for layer in range(2):
        if layer == 0:
            spread = jnp.broadcast_to(own_rows, (columns, own_count, depth))
            others = None
        else:
            spread = jnp.broadcast_to(
                own_rows.reshape(2, half, depth), (columns // 2, 2, half, depth)
            ).reshape(columns, half, depth)
            others = other_weights
        gathered = exchange(spread, "tp")
        far = project(layer, True, place, gathered, norm_gain, weights, others, None)
        came = from_partner(far, "dp")
        near = project(layer, False, place, gathered, norm_gain, weights, others, came)
        near = near.reshape(-1, *near.shape[2:])
        arrived = exchange(near, "dp") if layer == 0 else exchange(near, both, pairs)
        mixed, held = advance(
            layer, width, arrived, lengths, decay_base, group_gain, folded, held,
            [] if layer else [other_out],
        )
        shared = jnp.broadcast_to(mixed.reshape(2, 1, half, LANES), (2, owners, half, LANES))
        shared = exchange(shared.reshape(2 * owners, half, LANES), both, pairs)
        product = project_out(
            layer, place, shared.reshape(2, owners, half, LANES), w_out, other_out,
            [] if layer else [other_weights],
        )
        summed = exchange(product, "tp").astype(jnp.float32)
        summed = jnp.sum(summed.reshape(columns // 2, 2, half, depth), 0)
        own_rows = (
            own_rows.astype(jnp.float32) + summed.reshape(own_count, depth)
        ).astype(jnp.bfloat16)
    new_states = jnp.swapaxes(held.reshape(blocks, seqs, HEAD // 2, heads, LANES), 2, 3)
    return (own_rows, new_states.reshape(states.shape))


def solution(mesh):
    placed = (
        P(("grp", "tp"), "dp"),
        P(("grp", "dp")),
        P(None, "dp"),
        P(None, "dp", "tp"),
        P(None, "dp", "tp"),
        P(None, "dp", "tp"),
        P(None, "dp", "tp"),
        P(None, "dp", "tp"),
        P(None, "dp", "tp"),
        P(None, "tp"),
        P(None, "tp"),
        P(None, "tp", "dp"),
        P(None, ("grp", "dp"), "tp", None),
    )
    return jax.shard_map(
        per_device,
        mesh=mesh,
        in_specs=placed,
        out_specs=(P(("grp", "tp"), "dp"), P(None, ("grp", "dp"), "tp", None)),
        check_vma=False,
    )
```

```python
import functools

import jax
import jax.numpy as jnp
from jax import lax
from jax.experimental import pallas as pl
from jax.experimental.pallas import tpu as pltpu
from jax.sharding import PartitionSpec as P


HEAD = 64
NEW = 4
LANES = 128

norm_epsilon = 1e-06
unit_epsilon = 0.00064
group_epsilon = 0.00064

VMEM = pl.BlockSpec(memory_space=pltpu.VMEM)
SMEM = pl.BlockSpec(memory_space=pltpu.SMEM)


def iota(shape, dim):
    return lax.broadcasted_iota(jnp.int32, shape, dim)


def split_dot(x, ones):
    high = x.astype(jnp.bfloat16)
    low = (x - high.astype(jnp.float32)).astype(jnp.bfloat16)
    return jnp.dot(high, ones, preferred_element_type=jnp.float32) + jnp.dot(
        low, ones, preferred_element_type=jnp.float32
    )


def squares_tail(row):
    pick = iota((8, LANES), 0)
    high = row.astype(jnp.bfloat16).astype(jnp.float32)
    return jnp.where(pick == 0, high, jnp.where(pick == 1, row - high, 0.0)).astype(jnp.bfloat16)


def project_kernel(far, place_ref, x_ref, gain_ref, *refs):
    out_ref = refs[-1]
    blocks, rows, depth = x_ref.shape
    half = rows // 2
    first_half = place_ref[0] == (1 if far else 0)
    x = x_ref[...].astype(jnp.float32)
    x = jnp.where(first_half, x[:, :half], x[:, half:]).reshape(blocks * half, depth)
    scaled = (x * gain_ref[0:1, :]).astype(jnp.bfloat16)
    squares = jnp.sum(x * x, -1, keepdims=True)
    eye = iota((half, LANES), 0) == iota((half, LANES), 1)
    for first in range(0, 6, 2):
        pair = jnp.concatenate([refs[first][0], refs[first + 1][0]], 1)
        product = jnp.dot(scaled, pair, preferred_element_type=jnp.float32)
        for side in range(2):
            part = product[:, side * LANES : (side + 1) * LANES].reshape(blocks, half, LANES)
            where = pl.ds((first + side) * half, half)
            if not far:
                part = part + refs[-2][:, where, :].astype(jnp.float32)
            out_ref[:, where, :] = part.astype(jnp.bfloat16)
    for block in range(blocks):
        row = jnp.sum(
            jnp.where(eye, squares[block * half : (block + 1) * half], 0.0), 0, keepdims=True
        )
        if not far:
            came = refs[-2][block, pl.ds(6 * half, 8), :].astype(jnp.float32)
            row = row + came[0:1] + came[1:2]
        out_ref[block, pl.ds(6 * half, 8), :] = squares_tail(row)


def project_pair_kernel(place_ref, x_ref, gain_ref, packed_ref, *refs):
    *weight_refs, other_ref, core_own_ref, core_other_ref, out_ref = refs
    column = place_ref[1]
    blocks, rows, both = x_ref.shape
    depth = both // 2
    x = x_ref[...].astype(jnp.float32).reshape(blocks * rows, both)
    core_gain = packed_ref[pl.ds(packed_ref.shape[0] - 16, 16), :].astype(jnp.float32)
    core_gain = core_gain[0:1] + core_gain[1:2] + core_gain[2:3]
    own_scaled = (x[:, :depth] * gain_ref[1:2, :]).astype(jnp.bfloat16)
    core_scaled = (x[:, depth:] * core_gain).astype(jnp.bfloat16)
    squares = jnp.sum(x * x, -1, keepdims=True)
    eye = iota((rows, LANES), 0) == iota((rows, LANES), 1)
    for group in range(2):
        member = jnp.bitwise_xor(column, group)
        for first in range(0, 6, 2):
            if group:
                near = [other_ref[first], other_ref[first + 1]]
                core = [core_other_ref[first], core_other_ref[first + 1]]
            else:
                near = [weight_refs[first][1], weight_refs[first + 1][1]]
                core = [core_own_ref[first], core_own_ref[first + 1]]
            product = jnp.dot(
                own_scaled, jnp.concatenate(near, 1), preferred_element_type=jnp.float32
            ) + jnp.dot(core_scaled, jnp.concatenate(core, 1), preferred_element_type=jnp.float32)
            for side in range(2):
                part = product[:, side * LANES : (side + 1) * LANES]
                out_ref[member, :, pl.ds((first + side) * rows, rows), :] = part.reshape(
                    blocks, rows, LANES
                ).astype(jnp.bfloat16)
        for block in range(blocks):
            row = jnp.sum(
                jnp.where(eye, squares[block * rows : (block + 1) * rows], 0.0), 0, keepdims=True
            )
            out_ref[member, block, pl.ds(6 * rows, 8), :] = squares_tail(row)


def advance_kernel(layer, rows, width, arrived_ref, lengths_ref, base_ref, gain_ref, state_ref, *refs):
    mixed_ref, new_ref, line_ref, read_ref = refs[-4:]
    seqs = rows // NEW
    parts, part_rows = arrived_ref.shape[0], (arrived_ref.shape[1] - 8) // 6
    eye = iota((part_rows, LANES), 0) == iota((part_rows, LANES), 1)
    scaled = []
    for part in range(rows // part_rows):
        outer, core = part // 2, part % 2
        chips = parts * part_rows // rows
        total = arrived_ref[outer * chips * 2 + core].astype(jnp.float32)
        for chip in range(1, chips):
            total += arrived_ref[(outer * chips + chip) * 2 + core].astype(jnp.float32)
        square = total[6 * part_rows : 6 * part_rows + 1] + total[6 * part_rows + 1 : 6 * part_rows + 2]
        square = jnp.sum(jnp.where(eye, square, 0.0), 1, keepdims=True)
        inv_rms = lax.rsqrt(square / width + norm_epsilon)
        scaled.append(
            [inv_rms * total[role * part_rows : (role + 1) * part_rows] for role in range(6)]
        )
    recept, keys, values, decay_pre, rate_pre, gate_pre = [
        jnp.concatenate([part[role] for part in scaled], 0).astype(jnp.bfloat16).astype(jnp.float32)
        for role in range(6)
    ]
    same_head = (iota((LANES, LANES), 0) // HEAD == iota((LANES, LANES), 1) // HEAD).astype(
        jnp.float32
    ).astype(jnp.bfloat16)
    log_rate = base_ref[layer : layer + 1, :] + decay_pre
    decays = jnp.exp(jax.nn.sigmoid(log_rate) * (-0.6065306597126334))
    rates = jax.nn.sigmoid(rate_pre)
    unit = keys * lax.rsqrt(split_dot(keys * keys, same_head) + unit_epsilon)
    slot = iota((rows, LANES), 0)
    limit = jnp.zeros((rows, LANES), jnp.int32)
    for seq in range(seqs):
        limit = jnp.where(slot // NEW == seq, lengths_ref[seq], limit)
    live = slot % NEW < limit
    decays = jnp.where(live, decays, 1.0)
    unit = jnp.where(live, unit, 0.0)
    keys = jnp.where(live, keys, 0.0)
    lane = iota((rows, LANES), 1)
    for place, line in enumerate((decays, unit, unit * rates, keys, recept)):
        turned = pltpu.roll(line, HEAD, 1)
        line_ref[2 * place] = jnp.where(lane < HEAD, line, turned)
        line_ref[2 * place + 1] = jnp.where(lane < HEAD, turned, line)
    line_ref[10] = values
    even = iota((8, LANES), 0) % 2 == 0
    block_row, block_lane = iota((HEAD, LANES), 0), iota((HEAD, LANES), 1)
    place_mask = (block_row % 2 == block_lane // HEAD) & (block_row // 2 == block_lane % HEAD // 2)
    parity = (iota((LANES, LANES), 0) % 2 == iota((LANES, LANES), 1) // HEAD).astype(
        jnp.float32
    ).astype(jnp.bfloat16)
    parity_back = (iota((LANES, LANES), 1) % 2 == iota((LANES, LANES), 0) // HEAD).astype(
        jnp.float32
    ).astype(jnp.bfloat16)

    def spread(place, token):
        return jnp.where(
            even, line_ref[2 * place, pl.ds(token, 1), :], line_ref[2 * place + 1, pl.ds(token, 1), :]
        )[None]

    state = [
        state_ref[pl.ds(seq * HEAD, HEAD), :].reshape(8, 8, LANES) for seq in range(seqs)
    ]
    for position in range(NEW):
        tokens = [seq * NEW + position for seq in range(seqs)]
        against = jnp.concatenate(
            [(s * spread(1, t)).reshape(HEAD, LANES) for s, t in zip(state, tokens)], 0
        )
        removed = jnp.dot(
            against.astype(jnp.bfloat16), same_head, preferred_element_type=jnp.float32
        )
        written = jnp.concatenate(
            [jnp.where(place_mask, line_ref[10, pl.ds(t, 1), :], 0.0) for t in tokens], 0
        ).astype(jnp.bfloat16)
        written = jnp.dot(written, parity, preferred_element_type=jnp.float32)
        for seq, t in enumerate(tokens):
            part = slice(seq * HEAD, (seq + 1) * HEAD)
            state[seq] = (
                state[seq] * spread(0, t)
                - removed[part].reshape(8, 8, LANES) * spread(2, t)
                + written[part].reshape(8, 8, LANES) * spread(3, t)
            )
        read = jnp.concatenate(
            [(s * spread(4, t)).reshape(HEAD, LANES) for s, t in zip(state, tokens)], 0
        )
        read = jnp.dot(
            read.astype(jnp.bfloat16), parity_back, preferred_element_type=jnp.float32
        )
        for seq, t in enumerate(tokens):
            part = slice(seq * HEAD, (seq + 1) * HEAD)
            read_ref[pl.ds(t, 1), :] = jnp.sum(
                jnp.where(place_mask, read[part], 0.0), 0, keepdims=True
            )
    for seq in range(seqs):
        new_ref[0, pl.ds(seq * HEAD, HEAD), :] = state[seq].reshape(HEAD, LANES)
    read = read_ref[...]
    centred = read - split_dot(read, same_head) / HEAD
    variance = split_dot(centred * centred, same_head) / HEAD
    normed = centred * lax.rsqrt(variance + group_epsilon) * gain_ref[layer : layer + 1, :]
    mixed = jnp.where(live, normed * jax.nn.sigmoid(gate_pre), 0.0)
    members, owners, share, _ = mixed_ref.shape
    for member in range(members):
        for owner in range(owners):
            start = member * (rows // members) + (owner % 2) * share * (share * members < rows)
            mixed_ref[member, owner] = mixed[start : start + share].astype(jnp.bfloat16)


def out_kernel(layer, place_ref, mixed_ref, own_ref, other_ref, *refs):
    out_ref = refs[-1]
    _, blocks, rows, _ = mixed_ref.shape
    depth = own_ref.shape[2]
    first = place_ref[1] == 0
    sides = [(own_ref[layer], other_ref[layer])]
    if layer == 0:
        sides.append((refs[0][pl.ds(0, LANES), :], refs[0][pl.ds(LANES, LANES), :]))
    for side, (own, other) in enumerate(sides):
        total = 0.0
        for member, matrix in enumerate(
            (jnp.where(first, own, other), jnp.where(first, other, own))
        ):
            lines = mixed_ref[member].astype(jnp.float32).reshape(blocks * rows, LANES)
            total += jnp.dot(
                lines.astype(jnp.bfloat16), matrix, preferred_element_type=jnp.float32
            )
        out_ref[:, :, pl.ds(side * depth, depth)] = total.reshape(blocks, rows, depth).astype(
            jnp.bfloat16
        )


def settle_kernel(place_ref, summed_ref, tokens_ref, packed_ref, *refs):
    rows_ref, spread_ref = refs[-2:]
    columns, rows, _ = summed_ref.shape
    first = place_ref[0] == 0
    for member in range(2):
        total = summed_ref[member].astype(jnp.float32)
        for column in range(member + 2, columns, 2):
            total += summed_ref[column].astype(jnp.float32)
        near = tokens_ref[pl.ds(member * 2 * rows, 2 * rows), :].astype(jnp.float32)
        near = jnp.where(first, near[:rows], near[rows:])
        core = packed_ref[pl.ds(2 * LANES, 2 * rows), :].astype(jnp.float32)
        core = core[member * rows : (member + 1) * rows]
        total = (total + jnp.concatenate([near, core], 1)).astype(jnp.bfloat16)
        rows_ref[member] = total
        for column in range(member, columns, 2):
            spread_ref[column] = total


def finish_kernel(place_ref, summed_ref, rows_ref, back_ref, out_ref):
    columns, half, depth = summed_ref.shape
    first = place_ref[0] == 0
    for member in range(2):
        total = summed_ref[member].astype(jnp.float32)
        for column in range(member + 2, columns, 2):
            total += summed_ref[column].astype(jnp.float32)
        near = rows_ref[member].astype(jnp.float32)[:, :depth]
        core = back_ref[member].astype(jnp.float32)
        held = jnp.concatenate([jnp.where(first, near, core), jnp.where(first, core, near)], 0)
        out_ref[pl.ds(member * half, half), :] = (total + held).astype(jnp.bfloat16)


def params():
    return {
        "compiler_params": pltpu.CompilerParams(vmem_limit_bytes=24 * 2**20),
        "cost_estimate": pl.CostEstimate(
            flops=10**8, bytes_accessed=2 * 10**6, transcendentals=0
        ),
    }


def call(kernel, outs, *operands, awaited=()):
    return pl.pallas_call(
        kernel,
        out_shape=outs,
        in_specs=[SMEM]
        + [VMEM] * (len(operands) - 1)
        + [pl.BlockSpec(memory_space=pl.ANY)] * len(awaited),
        out_specs=jax.tree.map(lambda _: VMEM, outs),
        **params(),
    )(*operands, *awaited)


def bf16(*shape):
    return jax.ShapeDtypeStruct(shape, jnp.bfloat16)


def advance(layer, width, shared, arrived, lengths, base, gain, states, held, awaited):
    rows = lengths.shape[0] * NEW
    state_rows = states.shape[1]
    block = pl.BlockSpec((1, state_rows, LANES), lambda i: (layer, 0, 0))
    in_block = pl.BlockSpec((None, state_rows, LANES), lambda i: (layer, 0, 0))
    operands = [arrived, lengths, base, gain, states]
    in_specs = [VMEM, SMEM, VMEM, VMEM, in_block]
    aliases = {}
    if held is not None:
        aliases = {len(operands): 1}
        operands.append(held)
        in_specs.append(pl.BlockSpec(memory_space=pl.ANY))
    operands.extend(awaited)
    in_specs.extend([pl.BlockSpec(memory_space=pl.ANY)] * len(awaited))
    return pl.pallas_call(
        functools.partial(advance_kernel, layer, rows, width),
        grid=(1,),
        out_shape=(
            jax.ShapeDtypeStruct(shared, jnp.bfloat16),
            jax.ShapeDtypeStruct(states.shape, jnp.float32),
        ),
        in_specs=in_specs,
        out_specs=(pl.BlockSpec(shared, lambda i: (0, 0, 0, 0)), block),
        scratch_shapes=[
            pltpu.VMEM((11, rows, LANES), jnp.float32),
            pltpu.VMEM((rows, LANES), jnp.float32),
        ],
        input_output_aliases=aliases,
        **params(),
    )(*operands)


def exchange(x, axis, groups=None):
    return lax.all_to_all(x, axis, 0, 0, tiled=True, axis_index_groups=groups)


def from_partner(x, axis):
    return lax.ppermute(x, axis, [(i, i ^ 1) for i in range(lax.axis_size(axis))])


def per_device(
    tokens,
    lengths,
    norm_gain,
    w_recept,
    w_keys,
    w_values,
    w_decay,
    w_rate,
    w_gate,
    decay_base,
    group_gain,
    w_out,
    states,
):
    weights = (w_recept, w_keys, w_values, w_decay, w_rate, w_gate)
    own_count, depth = tokens.shape
    width = depth * lax.axis_size("dp")
    blocks, seqs, heads, _ = states.shape
    folded = states.reshape(blocks, seqs, heads, HEAD // 2, LANES)
    folded = jnp.swapaxes(folded, 2, 3).reshape(blocks, seqs * HEAD, LANES)
    columns, owners = lax.axis_size("tp"), lax.axis_size("dp")
    place = jnp.stack([lax.axis_index("dp") % 2, lax.axis_index("tp") % 2])
    both = ("tp", "dp")
    pairs = [
        [column * owners + owner for column in (first, first + 1) for owner in range(owners)]
        for first in range(0, columns, 2)
    ]
    half, quarter = own_count // 2, own_count // 4
    core = place[0]
    gathered = exchange(jnp.broadcast_to(tokens, (columns, own_count, depth)), "tp")
    other_out = from_partner(w_out, "tp")
    own_weights = jnp.stack([weight[1] for weight in weights])
    other_weights = from_partner(own_weights, "tp")
    quarters = tokens.reshape(2, 2, quarter, depth)
    quarters = jnp.where(core == 0, quarters[:, 1], quarters[:, 0])
    gain_line = norm_gain[1:2]
    gain_lines = []
    for _ in range(3):
        term = lax.reduce_precision(gain_line, 8, 7)
        gain_lines.append(term.astype(jnp.bfloat16))
        gain_line = gain_line - term
    packed = jnp.concatenate(
        [
            w_out[0],
            other_out[0],
            quarters.reshape(half, depth),
            *gain_lines,
            jnp.zeros((13, depth), jnp.bfloat16),
        ],
        0,
    )
    packed = from_partner(packed, "dp")
    core_own = from_partner(own_weights, "dp")
    core_other = from_partner(other_weights, "dp")
    far = call(
        functools.partial(project_kernel, True),
        bf16(columns, 3 * own_count + 8, LANES),
        place, gathered, norm_gain, *weights,
    )
    came = from_partner(far, "dp")
    near = call(
        functools.partial(project_kernel, False),
        bf16(columns, 3 * own_count + 8, LANES),
        place, gathered, norm_gain, *weights, came,
    )
    arrived = exchange(near, "dp")
    shared, held = advance(
        0, width, (2, owners, quarter, LANES), arrived, lengths, decay_base, group_gain,
        folded, None, [other_out],
    )
    shared = exchange(shared.reshape(2 * owners, quarter, LANES), both, pairs)
    product = call(
        functools.partial(out_kernel, 0),
        bf16(columns, quarter, 2 * depth),
        place, shared.reshape(2, owners, quarter, LANES), w_out, other_out, packed,
        awaited=[other_weights],
    )
    summed = exchange(product, "tp")
    rows, spread = call(
        settle_kernel,
        (bf16(2, quarter, 2 * depth), bf16(columns, quarter, 2 * depth)),
        place, summed, tokens, packed,
        awaited=[core_own, core_other],
    )
    gathered = exchange(spread, "tp")
    near = call(
        project_pair_kernel,
        bf16(2, columns, 6 * quarter + 8, LANES),
        place, gathered, norm_gain, packed, *weights, other_weights, core_own, core_other,
    )
    arrived = exchange(near.reshape(-1, *near.shape[2:]), both, pairs)
    back = from_partner(rows[:, :, depth:], "dp")
    shared, held = advance(
        1, width, (2, owners, half, LANES), arrived, lengths, decay_base, group_gain,
        folded, held, [],
    )
    shared = exchange(shared.reshape(2 * owners, half, LANES), both, pairs)
    product = call(
        functools.partial(out_kernel, 1),
        bf16(columns, half, depth),
        place, shared.reshape(2, owners, half, LANES), w_out, other_out,
    )
    summed = exchange(product, "tp")
    own_rows = call(finish_kernel, bf16(own_count, depth), place, summed, rows, back)
    new_states = jnp.swapaxes(held.reshape(blocks, seqs, HEAD // 2, heads, LANES), 2, 3)
    return (own_rows, new_states.reshape(states.shape))


def solution(mesh):
    placed = (
        P(("grp", "tp"), "dp"),
        P(("grp", "dp")),
        P(None, "dp"),
        P(None, "dp", "tp"),
        P(None, "dp", "tp"),
        P(None, "dp", "tp"),
        P(None, "dp", "tp"),
        P(None, "dp", "tp"),
        P(None, "dp", "tp"),
        P(None, "tp"),
        P(None, "tp"),
        P(None, "tp", "dp"),
        P(None, ("grp", "dp"), "tp", None),
    )
    return jax.shard_map(
        per_device,
        mesh=mesh,
        in_specs=placed,
        out_specs=(P(("grp", "tp"), "dp"), P(None, ("grp", "dp"), "tp", None)),
        check_vma=False,
    )
```

```python
import functools

import jax
import jax.numpy as jnp
from jax import lax
from jax.experimental import pallas as pl
from jax.experimental.pallas import tpu as pltpu
from jax.sharding import PartitionSpec as P


HEAD = 64
NEW = 4
LANES = 128

norm_epsilon = 1e-06
unit_epsilon = 0.00064
group_epsilon = 0.00064

VMEM = pl.BlockSpec(memory_space=pltpu.VMEM)


def place():
    return lax.rem(lax.axis_index("dp"), 2), lax.rem(lax.axis_index("tp"), 2)


def iota(shape, dim):
    return lax.broadcasted_iota(jnp.int32, shape, dim)


def split_dot(x, ones):
    high = x.astype(jnp.bfloat16)
    low = (x - high.astype(jnp.float32)).astype(jnp.bfloat16)
    return jnp.dot(high, ones, preferred_element_type=jnp.float32) + jnp.dot(
        low, ones, preferred_element_type=jnp.float32
    )


def squares_tail(row):
    pick = iota((8, LANES), 0)
    high = row.astype(jnp.bfloat16).astype(jnp.float32)
    return jnp.where(pick == 0, high, jnp.where(pick == 1, row - high, 0.0)).astype(jnp.bfloat16)


def project_kernel(far, x_ref, gain_ref, *refs):
    out_ref = refs[-1]
    blocks, rows, depth = x_ref.shape
    half = rows // 2
    first_half = place()[0] == (1 if far else 0)
    x = x_ref[...].astype(jnp.float32)
    x = jnp.where(first_half, x[:, :half], x[:, half:]).reshape(blocks * half, depth)
    scaled = (x * gain_ref[0:1, :]).astype(jnp.bfloat16)
    squares = jnp.sum(x * x, -1, keepdims=True)
    eye = iota((half, LANES), 0) == iota((half, LANES), 1)
    for first in range(0, 6, 2):
        pair = jnp.concatenate([refs[first][0], refs[first + 1][0]], 1)
        product = jnp.dot(scaled, pair, preferred_element_type=jnp.float32)
        for side in range(2):
            part = product[:, side * LANES : (side + 1) * LANES].reshape(blocks, half, LANES)
            where = pl.ds((first + side) * half, half)
            if not far:
                part = part + refs[-2][:, where, :].astype(jnp.float32)
            out_ref[:, where, :] = part.astype(jnp.bfloat16)
    for block in range(blocks):
        row = jnp.sum(
            jnp.where(eye, squares[block * half : (block + 1) * half], 0.0), 0, keepdims=True
        )
        if not far:
            came = refs[-2][block, pl.ds(6 * half, 8), :].astype(jnp.float32)
            row = row + came[0:1] + came[1:2]
        out_ref[block, pl.ds(6 * half, 8), :] = squares_tail(row)


def project_pair_kernel(x_ref, gain_ref, packed_ref, *refs):
    *weight_refs, other_ref, core_own_ref, core_other_ref, out_ref = refs
    column = place()[1]
    blocks, rows, both = x_ref.shape
    depth = both // 2
    x = x_ref[...].astype(jnp.float32).reshape(blocks * rows, both)
    core_gain = packed_ref[pl.ds(packed_ref.shape[0] - 16, 16), :].astype(jnp.float32)
    core_gain = core_gain[0:1] + core_gain[1:2] + core_gain[2:3]
    own_scaled = (x[:, :depth] * gain_ref[1:2, :]).astype(jnp.bfloat16)
    core_scaled = (x[:, depth:] * core_gain).astype(jnp.bfloat16)
    squares = jnp.sum(x * x, -1, keepdims=True)
    eye = iota((rows, LANES), 0) == iota((rows, LANES), 1)
    for group in range(2):
        member = jnp.bitwise_xor(column, group)
        for first in range(0, 6, 2):
            if group:
                near = [other_ref[first], other_ref[first + 1]]
                core = [core_other_ref[first], core_other_ref[first + 1]]
            else:
                near = [weight_refs[first][1], weight_refs[first + 1][1]]
                core = [core_own_ref[first], core_own_ref[first + 1]]
            product = jnp.dot(
                own_scaled, jnp.concatenate(near, 1), preferred_element_type=jnp.float32
            ) + jnp.dot(core_scaled, jnp.concatenate(core, 1), preferred_element_type=jnp.float32)
            for side in range(2):
                part = product[:, side * LANES : (side + 1) * LANES]
                out_ref[member, :, pl.ds((first + side) * rows, rows), :] = part.reshape(
                    blocks, rows, LANES
                ).astype(jnp.bfloat16)
        for block in range(blocks):
            row = jnp.sum(
                jnp.where(eye, squares[block * rows : (block + 1) * rows], 0.0), 0, keepdims=True
            )
            out_ref[member, block, pl.ds(6 * rows, 8), :] = squares_tail(row)


def advance_kernel(layer, rows, width, arrived_ref, limits_ref, base_ref, gain_ref, state_ref, *refs):
    mixed_ref, new_ref, line_ref, read_ref = refs[-4:]
    seqs = rows // NEW
    parts, part_rows = arrived_ref.shape[0], (arrived_ref.shape[1] - 8) // 6
    eye = iota((part_rows, LANES), 0) == iota((part_rows, LANES), 1)
    scaled = []
    for part in range(rows // part_rows):
        outer, core = part // 2, part % 2
        chips = parts * part_rows // rows
        total = arrived_ref[outer * chips * 2 + core].astype(jnp.float32)
        for chip in range(1, chips):
            total += arrived_ref[(outer * chips + chip) * 2 + core].astype(jnp.float32)
        square = total[6 * part_rows : 6 * part_rows + 1] + total[6 * part_rows + 1 : 6 * part_rows + 2]
        square = jnp.sum(jnp.where(eye, square, 0.0), 1, keepdims=True)
        inv_rms = lax.rsqrt(square / width + norm_epsilon)
        scaled.append(
            [inv_rms * total[role * part_rows : (role + 1) * part_rows] for role in range(6)]
        )
    recept, keys, values, decay_pre, rate_pre, gate_pre = [
        jnp.concatenate([part[role] for part in scaled], 0).astype(jnp.bfloat16).astype(jnp.float32)
        for role in range(6)
    ]
    same_head = (iota((LANES, LANES), 0) // HEAD == iota((LANES, LANES), 1) // HEAD).astype(
        jnp.float32
    ).astype(jnp.bfloat16)
    log_rate = base_ref[layer : layer + 1, :] + decay_pre
    decays = jnp.exp(jax.nn.sigmoid(log_rate) * (-0.6065306597126334))
    rates = jax.nn.sigmoid(rate_pre)
    unit = keys * lax.rsqrt(split_dot(keys * keys, same_head) + unit_epsilon)
    live = iota((rows, LANES), 0) % NEW < limits_ref[...]
    decays = jnp.where(live, decays, 1.0)
    unit = jnp.where(live, unit, 0.0)
    keys = jnp.where(live, keys, 0.0)
    lane = iota((rows, LANES), 1)
    for place, line in enumerate((decays, unit, unit * rates, keys, recept)):
        turned = pltpu.roll(line, HEAD, 1)
        line_ref[2 * place] = jnp.where(lane < HEAD, line, turned)
        line_ref[2 * place + 1] = jnp.where(lane < HEAD, turned, line)
    line_ref[10] = values
    even = iota((8, LANES), 0) % 2 == 0
    block_row, block_lane = iota((HEAD, LANES), 0), iota((HEAD, LANES), 1)
    place_mask = (block_row % 2 == block_lane // HEAD) & (block_row // 2 == block_lane % HEAD // 2)
    parity = (iota((LANES, LANES), 0) % 2 == iota((LANES, LANES), 1) // HEAD).astype(
        jnp.float32
    ).astype(jnp.bfloat16)
    parity_back = (iota((LANES, LANES), 1) % 2 == iota((LANES, LANES), 0) // HEAD).astype(
        jnp.float32
    ).astype(jnp.bfloat16)

    def spread(place, token):
        return jnp.where(
            even, line_ref[2 * place, pl.ds(token, 1), :], line_ref[2 * place + 1, pl.ds(token, 1), :]
        )[None]

    state = [
        state_ref[layer, pl.ds(seq * HEAD, HEAD), :].reshape(8, 8, LANES) for seq in range(seqs)
    ]
    for position in range(NEW):
        tokens = [seq * NEW + position for seq in range(seqs)]
        against = jnp.concatenate(
            [(s * spread(1, t)).reshape(HEAD, LANES) for s, t in zip(state, tokens)], 0
        )
        removed = jnp.dot(
            against.astype(jnp.bfloat16), same_head, preferred_element_type=jnp.float32
        )
        written = jnp.concatenate(
            [jnp.where(place_mask, line_ref[10, pl.ds(t, 1), :], 0.0) for t in tokens], 0
        ).astype(jnp.bfloat16)
        written = jnp.dot(written, parity, preferred_element_type=jnp.float32)
        for seq, t in enumerate(tokens):
            part = slice(seq * HEAD, (seq + 1) * HEAD)
            state[seq] = (
                state[seq] * spread(0, t)
                - removed[part].reshape(8, 8, LANES) * spread(2, t)
                + written[part].reshape(8, 8, LANES) * spread(3, t)
            )
        read = jnp.concatenate(
            [(s * spread(4, t)).reshape(HEAD, LANES) for s, t in zip(state, tokens)], 0
        )
        read = jnp.dot(
            read.astype(jnp.bfloat16), parity_back, preferred_element_type=jnp.float32
        )
        for seq, t in enumerate(tokens):
            part = slice(seq * HEAD, (seq + 1) * HEAD)
            read_ref[pl.ds(t, 1), :] = jnp.sum(
                jnp.where(place_mask, read[part], 0.0), 0, keepdims=True
            )
    for seq in range(seqs):
        new_ref[pl.ds(seq * HEAD, HEAD), :] = state[seq].reshape(HEAD, LANES)
    read = read_ref[...]
    centred = read - split_dot(read, same_head) / HEAD
    variance = split_dot(centred * centred, same_head) / HEAD
    normed = centred * lax.rsqrt(variance + group_epsilon) * gain_ref[layer : layer + 1, :]
    mixed = jnp.where(live, normed * jax.nn.sigmoid(gate_pre), 0.0)
    members, owners, share, _ = mixed_ref.shape
    for member in range(members):
        for owner in range(owners):
            start = member * (rows // members) + (owner % 2) * share * (share * members < rows)
            mixed_ref[member, owner] = mixed[start : start + share].astype(jnp.bfloat16)


def out_kernel(layer, mixed_ref, own_ref, other_ref, *refs):
    out_ref = refs[-1]
    _, blocks, rows, _ = mixed_ref.shape
    depth = own_ref.shape[2]
    first = place()[1] == 0
    sides = [(own_ref[layer], other_ref[layer])]
    if layer == 0:
        sides.append((refs[0][pl.ds(0, LANES), :], refs[0][pl.ds(LANES, LANES), :]))
    for side, (own, other) in enumerate(sides):
        total = 0.0
        for member, matrix in enumerate(
            (jnp.where(first, own, other), jnp.where(first, other, own))
        ):
            lines = mixed_ref[member].astype(jnp.float32).reshape(blocks * rows, LANES)
            total += jnp.dot(
                lines.astype(jnp.bfloat16), matrix, preferred_element_type=jnp.float32
            )
        out_ref[:, :, pl.ds(side * depth, depth)] = total.reshape(blocks, rows, depth).astype(
            jnp.bfloat16
        )


def settle_kernel(summed_ref, tokens_ref, packed_ref, *refs):
    rows_ref, spread_ref = refs[-2:]
    columns, rows, _ = summed_ref.shape
    first = place()[0] == 0
    for member in range(2):
        total = summed_ref[member].astype(jnp.float32)
        for column in range(member + 2, columns, 2):
            total += summed_ref[column].astype(jnp.float32)
        near = tokens_ref[pl.ds(member * 2 * rows, 2 * rows), :].astype(jnp.float32)
        near = jnp.where(first, near[:rows], near[rows:])
        core = packed_ref[pl.ds(2 * LANES, 2 * rows), :].astype(jnp.float32)
        core = core[member * rows : (member + 1) * rows]
        total = (total + jnp.concatenate([near, core], 1)).astype(jnp.bfloat16)
        rows_ref[member] = total
        for column in range(member, columns, 2):
            spread_ref[column] = total


def finish_kernel(summed_ref, rows_ref, back_ref, out_ref):
    columns, half, depth = summed_ref.shape
    first = place()[0] == 0
    for member in range(2):
        total = summed_ref[member].astype(jnp.float32)
        for column in range(member + 2, columns, 2):
            total += summed_ref[column].astype(jnp.float32)
        near = rows_ref[member].astype(jnp.float32)[:, :depth]
        core = back_ref[member].astype(jnp.float32)
        held = jnp.concatenate([jnp.where(first, near, core), jnp.where(first, core, near)], 0)
        out_ref[pl.ds(member * half, half), :] = (total + held).astype(jnp.bfloat16)


def params():
    return {
        "compiler_params": pltpu.CompilerParams(vmem_limit_bytes=24 * 2**20),
        "cost_estimate": pl.CostEstimate(
            flops=10**8, bytes_accessed=2 * 10**6, transcendentals=0
        ),
    }


def call(kernel, outs, *operands, awaited=()):
    return pl.pallas_call(
        kernel,
        out_shape=outs,
        in_specs=[VMEM] * len(operands)
        + [pl.BlockSpec(memory_space=pl.ANY)] * len(awaited),
        out_specs=jax.tree.map(lambda _: VMEM, outs),
        **params(),
    )(*operands, *awaited)


def bf16(*shape):
    return jax.ShapeDtypeStruct(shape, jnp.bfloat16)


def advance(layer, width, shared, arrived, limits, base, gain, states, awaited):
    rows = limits.shape[0]
    return pl.pallas_call(
        functools.partial(advance_kernel, layer, rows, width),
        out_shape=(bf16(*shared), jax.ShapeDtypeStruct(states.shape[1:], jnp.float32)),
        in_specs=[VMEM] * 5 + [pl.BlockSpec(memory_space=pl.ANY)] * len(awaited),
        out_specs=(VMEM, VMEM),
        scratch_shapes=[
            pltpu.VMEM((11, rows, LANES), jnp.float32),
            pltpu.VMEM((rows, LANES), jnp.float32),
        ],
        **params(),
    )(arrived, limits, base, gain, states, *awaited)


def exchange(x, axis, groups=None):
    return lax.all_to_all(x, axis, 0, 0, tiled=True, axis_index_groups=groups)


def from_partner(x, axis):
    return lax.ppermute(x, axis, [(i, i ^ 1) for i in range(lax.axis_size(axis))])


def per_device(
    tokens,
    lengths,
    norm_gain,
    w_recept,
    w_keys,
    w_values,
    w_decay,
    w_rate,
    w_gate,
    decay_base,
    group_gain,
    w_out,
    states,
):
    weights = (w_recept, w_keys, w_values, w_decay, w_rate, w_gate)
    own_count, depth = tokens.shape
    width = depth * lax.axis_size("dp")
    blocks, seqs, heads, _ = states.shape
    folded = states.reshape(blocks, seqs, heads, HEAD // 2, LANES)
    folded = jnp.swapaxes(folded, 2, 3).reshape(blocks, seqs * HEAD, LANES)
    columns, owners = lax.axis_size("tp"), lax.axis_size("dp")
    both = ("tp", "dp")
    pairs = [
        [column * owners + owner for column in (first, first + 1) for owner in range(owners)]
        for first in range(0, columns, 2)
    ]
    half, quarter = own_count // 2, own_count // 4
    core = place()[0]
    limits = jnp.broadcast_to(jnp.repeat(lengths, NEW)[:, None], (own_count, LANES))
    gathered = exchange(jnp.broadcast_to(tokens, (columns, own_count, depth)), "tp")
    other_out = from_partner(w_out, "tp")
    own_weights = jnp.stack([weight[1] for weight in weights])
    other_weights = from_partner(own_weights, "tp")
    quarters = tokens.reshape(2, 2, quarter, depth)
    quarters = jnp.where(core == 0, quarters[:, 1], quarters[:, 0])
    gain_line = norm_gain[1:2]
    gain_lines = []
    for _ in range(3):
        term = lax.reduce_precision(gain_line, 8, 7)
        gain_lines.append(term.astype(jnp.bfloat16))
        gain_line = gain_line - term
    packed = jnp.concatenate(
        [
            w_out[0],
            other_out[0],
            quarters.reshape(half, depth),
            *gain_lines,
            jnp.zeros((13, depth), jnp.bfloat16),
        ],
        0,
    )
    packed = from_partner(packed, "dp")
    core_own = from_partner(own_weights, "dp")
    core_other = from_partner(other_weights, "dp")
    far = call(
        functools.partial(project_kernel, True),
        bf16(columns, 3 * own_count + 8, LANES),
        gathered, norm_gain, *weights,
    )
    came = from_partner(far, "dp")
    near = call(
        functools.partial(project_kernel, False),
        bf16(columns, 3 * own_count + 8, LANES),
        gathered, norm_gain, *weights, came,
    )
    arrived = exchange(near, "dp")
    shared, first_states = advance(
        0, width, (2, owners, quarter, LANES), arrived, limits, decay_base, group_gain,
        folded, [other_out],
    )
    shared = exchange(shared.reshape(2 * owners, quarter, LANES), both, pairs)
    product = call(
        functools.partial(out_kernel, 0),
        bf16(columns, quarter, 2 * depth),
        shared.reshape(2, owners, quarter, LANES), w_out, other_out, packed,
        awaited=[other_weights],
    )
    summed = exchange(product, "tp")
    rows, spread = call(
        settle_kernel,
        (bf16(2, quarter, 2 * depth), bf16(columns, quarter, 2 * depth)),
        summed, tokens, packed,
        awaited=[core_own, core_other],
    )
    gathered = exchange(spread, "tp")
    near = call(
        project_pair_kernel,
        bf16(2, columns, 6 * quarter + 8, LANES),
        gathered, norm_gain, packed, *weights, other_weights, core_own, core_other,
    )
    arrived = exchange(near.reshape(-1, *near.shape[2:]), both, pairs)
    back = from_partner(rows[:, :, depth:], "dp")
    shared, last_states = advance(
        1, width, (2, owners, half, LANES), arrived, limits, decay_base, group_gain,
        folded, [],
    )
    shared = exchange(shared.reshape(2 * owners, half, LANES), both, pairs)
    product = call(
        functools.partial(out_kernel, 1),
        bf16(columns, half, depth),
        shared.reshape(2, owners, half, LANES), w_out, other_out,
    )
    summed = exchange(product, "tp")
    own_rows = call(finish_kernel, bf16(own_count, depth), summed, rows, back)
    held = jnp.stack([first_states, last_states])
    new_states = jnp.swapaxes(held.reshape(blocks, seqs, HEAD // 2, heads, LANES), 2, 3)
    return (own_rows, new_states.reshape(states.shape))


def solution(mesh):
    placed = (
        P(("grp", "tp"), "dp"),
        P(("grp", "dp")),
        P(None, "dp"),
        P(None, "dp", "tp"),
        P(None, "dp", "tp"),
        P(None, "dp", "tp"),
        P(None, "dp", "tp"),
        P(None, "dp", "tp"),
        P(None, "dp", "tp"),
        P(None, "tp"),
        P(None, "tp"),
        P(None, "tp", "dp"),
        P(None, ("grp", "dp"), "tp", None),
    )
    return jax.shard_map(
        per_device,
        mesh=mesh,
        in_specs=placed,
        out_specs=(P(("grp", "tp"), "dp"), P(None, ("grp", "dp"), "tp", None)),
        check_vma=False,
    )
```

```python
import functools

import jax
import jax.numpy as jnp
from jax import lax
from jax.experimental import pallas as pl
from jax.experimental.pallas import tpu as pltpu
from jax.sharding import PartitionSpec as P


HEAD = 64
NEW = 4
LANES = 128

norm_epsilon = 1e-06
unit_epsilon = 0.00064
group_epsilon = 0.00064

VMEM = pl.BlockSpec(memory_space=pltpu.VMEM)


def place():
    return lax.rem(lax.axis_index("dp"), 2), lax.rem(lax.axis_index("tp"), 2)


def iota(shape, dim):
    return lax.broadcasted_iota(jnp.int32, shape, dim)


def split_dot(x, ones):
    high = x.astype(jnp.bfloat16)
    low = (x - high.astype(jnp.float32)).astype(jnp.bfloat16)
    return jnp.dot(high, ones, preferred_element_type=jnp.float32) + jnp.dot(
        low, ones, preferred_element_type=jnp.float32
    )


def squares_tail(row):
    pick = iota((8, LANES), 0)
    high = row.astype(jnp.bfloat16).astype(jnp.float32)
    return jnp.where(pick == 0, high, jnp.where(pick == 1, row - high, 0.0)).astype(jnp.bfloat16)


def project_kernel(far, x_ref, gain_ref, *refs):
    out_ref = refs[-1]
    blocks, rows, depth = x_ref.shape
    half = rows // 2
    first_half = place()[0] == (1 if far else 0)
    x = x_ref[...].astype(jnp.float32)
    x = jnp.where(first_half, x[:, :half], x[:, half:]).reshape(blocks * half, depth)
    scaled = (x * gain_ref[0:1, :]).astype(jnp.bfloat16)
    squares = jnp.sum(x * x, -1, keepdims=True)
    eye = iota((half, LANES), 0) == iota((half, LANES), 1)
    for first in range(0, 6, 2):
        pair = jnp.concatenate([refs[first][0], refs[first + 1][0]], 1)
        product = jnp.dot(scaled, pair, preferred_element_type=jnp.float32)
        for side in range(2):
            part = product[:, side * LANES : (side + 1) * LANES].reshape(blocks, half, LANES)
            where = pl.ds((first + side) * half, half)
            if not far:
                part = part + refs[-2][:, where, :].astype(jnp.float32)
            out_ref[:, where, :] = part.astype(jnp.bfloat16)
    for block in range(blocks):
        row = jnp.sum(
            jnp.where(eye, squares[block * half : (block + 1) * half], 0.0), 0, keepdims=True
        )
        if not far:
            came = refs[-2][block, pl.ds(6 * half, 8), :].astype(jnp.float32)
            row = row + came[0:1] + came[1:2]
        out_ref[block, pl.ds(6 * half, 8), :] = squares_tail(row)


def project_pair_kernel(x_ref, gain_ref, packed_ref, *refs):
    *weight_refs, other_ref, core_own_ref, core_other_ref, out_ref = refs
    column = place()[1]
    blocks, rows, both = x_ref.shape
    depth = both // 2
    x = x_ref[...].astype(jnp.float32).reshape(blocks * rows, both)
    core_gain = packed_ref[pl.ds(packed_ref.shape[0] - 16, 16), :].astype(jnp.float32)
    core_gain = core_gain[0:1] + core_gain[1:2] + core_gain[2:3]
    own_scaled = (x[:, :depth] * gain_ref[1:2, :]).astype(jnp.bfloat16)
    core_scaled = (x[:, depth:] * core_gain).astype(jnp.bfloat16)
    squares = jnp.sum(x * x, -1, keepdims=True)
    eye = iota((rows, LANES), 0) == iota((rows, LANES), 1)
    for group in range(2):
        member = jnp.bitwise_xor(column, group)
        for first in range(0, 6, 2):
            if group:
                near = [other_ref[first], other_ref[first + 1]]
                core = [core_other_ref[first], core_other_ref[first + 1]]
            else:
                near = [weight_refs[first][1], weight_refs[first + 1][1]]
                core = [core_own_ref[first], core_own_ref[first + 1]]
            product = jnp.dot(
                own_scaled, jnp.concatenate(near, 1), preferred_element_type=jnp.float32
            ) + jnp.dot(core_scaled, jnp.concatenate(core, 1), preferred_element_type=jnp.float32)
            for side in range(2):
                part = product[:, side * LANES : (side + 1) * LANES]
                out_ref[member, :, pl.ds((first + side) * rows, rows), :] = part.reshape(
                    blocks, rows, LANES
                ).astype(jnp.bfloat16)
        for block in range(blocks):
            row = jnp.sum(
                jnp.where(eye, squares[block * rows : (block + 1) * rows], 0.0), 0, keepdims=True
            )
            out_ref[member, block, pl.ds(6 * rows, 8), :] = squares_tail(row)


def advance_kernel(layer, rows, width, arrived_ref, limits_ref, base_ref, gain_ref, state_ref, *refs):
    mixed_ref, new_ref, line_ref, read_ref = refs[-4:]
    seqs = rows // NEW
    parts, part_rows = arrived_ref.shape[0], (arrived_ref.shape[1] - 8) // 6
    eye = iota((part_rows, LANES), 0) == iota((part_rows, LANES), 1)
    scaled = []
    for part in range(rows // part_rows):
        outer, core = part // 2, part % 2
        chips = parts * part_rows // rows
        total = arrived_ref[outer * chips * 2 + core].astype(jnp.float32)
        for chip in range(1, chips):
            total += arrived_ref[(outer * chips + chip) * 2 + core].astype(jnp.float32)
        square = total[6 * part_rows : 6 * part_rows + 1] + total[6 * part_rows + 1 : 6 * part_rows + 2]
        square = jnp.sum(jnp.where(eye, square, 0.0), 1, keepdims=True)
        inv_rms = lax.rsqrt(square / width + norm_epsilon)
        scaled.append(
            [inv_rms * total[role * part_rows : (role + 1) * part_rows] for role in range(6)]
        )
    recept, keys, values, decay_pre, rate_pre, gate_pre = [
        jnp.concatenate([part[role] for part in scaled], 0).astype(jnp.bfloat16).astype(jnp.float32)
        for role in range(6)
    ]
    same_head = (iota((LANES, LANES), 0) // HEAD == iota((LANES, LANES), 1) // HEAD).astype(
        jnp.float32
    ).astype(jnp.bfloat16)
    log_rate = base_ref[layer : layer + 1, :] + decay_pre
    decays = jnp.exp(jax.nn.sigmoid(log_rate) * (-0.6065306597126334))
    rates = jax.nn.sigmoid(rate_pre)
    unit = keys * lax.rsqrt(split_dot(keys * keys, same_head) + unit_epsilon)
    seqs_row = limits_ref[...].astype(jnp.float32)
    of_seq = iota((rows, seqs), 0) // NEW == iota((rows, seqs), 1)
    limit = jnp.sum(jnp.where(of_seq, seqs_row, 0.0), 1, keepdims=True)
    live = (iota((rows, LANES), 0) % NEW).astype(jnp.float32) < limit
    decays = jnp.where(live, decays, 1.0)
    unit = jnp.where(live, unit, 0.0)
    keys = jnp.where(live, keys, 0.0)
    lane = iota((rows, LANES), 1)
    for place, line in enumerate((decays, unit, unit * rates, keys, recept)):
        turned = pltpu.roll(line, HEAD, 1)
        line_ref[2 * place] = jnp.where(lane < HEAD, line, turned)
        line_ref[2 * place + 1] = jnp.where(lane < HEAD, turned, line)
    line_ref[10] = values
    even = iota((8, LANES), 0) % 2 == 0
    block_row, block_lane = iota((HEAD, LANES), 0), iota((HEAD, LANES), 1)
    place_mask = (block_row % 2 == block_lane // HEAD) & (block_row // 2 == block_lane % HEAD // 2)
    parity = (iota((LANES, LANES), 0) % 2 == iota((LANES, LANES), 1) // HEAD).astype(
        jnp.float32
    ).astype(jnp.bfloat16)
    parity_back = (iota((LANES, LANES), 1) % 2 == iota((LANES, LANES), 0) // HEAD).astype(
        jnp.float32
    ).astype(jnp.bfloat16)

    def spread(place, token):
        return jnp.where(
            even, line_ref[2 * place, pl.ds(token, 1), :], line_ref[2 * place + 1, pl.ds(token, 1), :]
        )[None]

    state = [
        state_ref[layer, pl.ds(seq * HEAD, HEAD), :].reshape(8, 8, LANES) for seq in range(seqs)
    ]
    for position in range(NEW):
        tokens = [seq * NEW + position for seq in range(seqs)]
        against = jnp.concatenate(
            [(s * spread(1, t)).reshape(HEAD, LANES) for s, t in zip(state, tokens)], 0
        )
        removed = jnp.dot(
            against.astype(jnp.bfloat16), same_head, preferred_element_type=jnp.float32
        )
        written = jnp.concatenate(
            [jnp.where(place_mask, line_ref[10, pl.ds(t, 1), :], 0.0) for t in tokens], 0
        ).astype(jnp.bfloat16)
        written = jnp.dot(written, parity, preferred_element_type=jnp.float32)
        for seq, t in enumerate(tokens):
            part = slice(seq * HEAD, (seq + 1) * HEAD)
            state[seq] = (
                state[seq] * spread(0, t)
                - removed[part].reshape(8, 8, LANES) * spread(2, t)
                + written[part].reshape(8, 8, LANES) * spread(3, t)
            )
        read = jnp.concatenate(
            [(s * spread(4, t)).reshape(HEAD, LANES) for s, t in zip(state, tokens)], 0
        )
        read = jnp.dot(
            read.astype(jnp.bfloat16), parity_back, preferred_element_type=jnp.float32
        )
        for seq, t in enumerate(tokens):
            part = slice(seq * HEAD, (seq + 1) * HEAD)
            read_ref[pl.ds(t, 1), :] = jnp.sum(
                jnp.where(place_mask, read[part], 0.0), 0, keepdims=True
            )
    for seq in range(seqs):
        new_ref[pl.ds(seq * HEAD, HEAD), :] = state[seq].reshape(HEAD, LANES)
    read = read_ref[...]
    centred = read - split_dot(read, same_head) / HEAD
    variance = split_dot(centred * centred, same_head) / HEAD
    normed = centred * lax.rsqrt(variance + group_epsilon) * gain_ref[layer : layer + 1, :]
    mixed = jnp.where(live, normed * jax.nn.sigmoid(gate_pre), 0.0)
    members, owners, share, _ = mixed_ref.shape
    for member in range(members):
        for owner in range(owners):
            start = member * (rows // members) + (owner % 2) * share * (share * members < rows)
            mixed_ref[member, owner] = mixed[start : start + share].astype(jnp.bfloat16)


def out_kernel(layer, mixed_ref, own_ref, other_ref, *refs):
    out_ref = refs[-1]
    _, blocks, rows, _ = mixed_ref.shape
    depth = own_ref.shape[2]
    first = place()[1] == 0
    sides = [(own_ref[layer], other_ref[layer])]
    if layer == 0:
        sides.append((refs[0][pl.ds(0, LANES), :], refs[0][pl.ds(LANES, LANES), :]))
    for side, (own, other) in enumerate(sides):
        total = 0.0
        for member, matrix in enumerate(
            (jnp.where(first, own, other), jnp.where(first, other, own))
        ):
            lines = mixed_ref[member].astype(jnp.float32).reshape(blocks * rows, LANES)
            total += jnp.dot(
                lines.astype(jnp.bfloat16), matrix, preferred_element_type=jnp.float32
            )
        out_ref[:, :, pl.ds(side * depth, depth)] = total.reshape(blocks, rows, depth).astype(
            jnp.bfloat16
        )


def out_quad_kernel(mixed_ref, pair_ref, far_ref, out_ref):
    members, blocks, rows, _ = mixed_ref.shape
    me = lax.rem(lax.axis_index("tp"), members)
    total = 0.0
    for member in range(members):
        offset = jnp.bitwise_xor(me, member)
        side = lax.rem(offset, 2)
        matrix = jnp.where(offset < 2, pair_ref[side], far_ref[side])
        lines = mixed_ref[member].astype(jnp.float32).reshape(blocks * rows, LANES)
        total += jnp.dot(lines.astype(jnp.bfloat16), matrix, preferred_element_type=jnp.float32)
    out_ref[...] = total.reshape(blocks, rows, total.shape[1]).astype(jnp.bfloat16)


def stack_kernel(layer, *refs):
    for index, ref in enumerate(refs[:-1]):
        refs[-1][index] = ref[layer]


def pack_kernel(own_ref, other_ref, tokens_ref, gain_ref, out_ref):
    quarter = tokens_ref.shape[0] // 4
    out_ref[pl.ds(0, LANES), :] = own_ref[0]
    out_ref[pl.ds(LANES, LANES), :] = other_ref[0]
    lines = []
    for member in range(2):
        near = tokens_ref[pl.ds(member * 2 * quarter, 2 * quarter), :].astype(jnp.float32)
        lines.append(jnp.where(place()[0] == 0, near[quarter:], near[:quarter]))
    out_ref[pl.ds(2 * LANES, 2 * quarter), :] = jnp.concatenate(lines, 0).astype(jnp.bfloat16)
    rest = gain_ref[1:2, :]
    pick = iota((16, rest.shape[1]), 0)
    lines = jnp.zeros(pick.shape, jnp.float32)
    for index in range(3):
        term = rest.astype(jnp.bfloat16).astype(jnp.float32)
        lines = jnp.where(pick == index, term, lines)
        rest = rest - term
    out_ref[pl.ds(2 * LANES + 2 * quarter, 16), :] = lines.astype(jnp.bfloat16)


def settle_kernel(summed_ref, tokens_ref, packed_ref, *refs):
    rows_ref, spread_ref = refs[-2:]
    columns, rows, _ = summed_ref.shape
    first = place()[0] == 0
    for member in range(2):
        total = summed_ref[member].astype(jnp.float32)
        for column in range(member + 2, columns, 2):
            total += summed_ref[column].astype(jnp.float32)
        near = tokens_ref[pl.ds(member * 2 * rows, 2 * rows), :].astype(jnp.float32)
        near = jnp.where(first, near[:rows], near[rows:])
        core = packed_ref[pl.ds(2 * LANES, 2 * rows), :].astype(jnp.float32)
        core = core[member * rows : (member + 1) * rows]
        total = (total + jnp.concatenate([near, core], 1)).astype(jnp.bfloat16)
        rows_ref[member] = total
        for column in range(member, columns, 2):
            spread_ref[column] = total


def finish_kernel(summed_ref, rows_ref, back_ref, out_ref):
    columns, _, depth = summed_ref.shape
    first = place()[0] == 0
    lines = []
    for member in range(4):
        total = summed_ref[member].astype(jnp.float32)
        for column in range(member + 4, columns, 4):
            total += summed_ref[column].astype(jnp.float32)
        near = rows_ref[member // 2].astype(jnp.float32)[:, :depth]
        core = back_ref[member // 2].astype(jnp.float32)
        held = jnp.where(first, near, core) if member % 2 == 0 else jnp.where(first, core, near)
        lines.append(total + held)
    out_ref[...] = jnp.concatenate(lines, 0).astype(jnp.bfloat16)


def params():
    return {
        "compiler_params": pltpu.CompilerParams(vmem_limit_bytes=24 * 2**20),
        "cost_estimate": pl.CostEstimate(
            flops=10**8, bytes_accessed=2 * 10**6, transcendentals=0
        ),
    }


def call(kernel, outs, *operands, awaited=()):
    return pl.pallas_call(
        kernel,
        out_shape=outs,
        in_specs=[VMEM] * len(operands)
        + [pl.BlockSpec(memory_space=pl.ANY)] * len(awaited),
        out_specs=jax.tree.map(lambda _: VMEM, outs),
        **params(),
    )(*operands, *awaited)


def bf16(*shape):
    return jax.ShapeDtypeStruct(shape, jnp.bfloat16)


def advance(layer, width, shared, arrived, limits, base, gain, states, awaited):
    rows = limits.shape[1] * NEW
    return pl.pallas_call(
        functools.partial(advance_kernel, layer, rows, width),
        out_shape=(bf16(*shared), jax.ShapeDtypeStruct(states.shape[1:], jnp.float32)),
        in_specs=[VMEM] * 5 + [pl.BlockSpec(memory_space=pl.ANY)] * len(awaited),
        out_specs=(VMEM, VMEM),
        scratch_shapes=[
            pltpu.VMEM((11, rows, LANES), jnp.float32),
            pltpu.VMEM((rows, LANES), jnp.float32),
        ],
        **params(),
    )(arrived, limits, base, gain, states, *awaited)


def exchange(x, axis, groups=None):
    return lax.all_to_all(x, axis, 0, 0, tiled=True, axis_index_groups=groups)


def from_partner(x, axis):
    return lax.ppermute(x, axis, [(i, i ^ 1) for i in range(lax.axis_size(axis))])


def per_device(
    tokens,
    lengths,
    norm_gain,
    w_recept,
    w_keys,
    w_values,
    w_decay,
    w_rate,
    w_gate,
    decay_base,
    group_gain,
    w_out,
    states,
):
    weights = (w_recept, w_keys, w_values, w_decay, w_rate, w_gate)
    own_count, depth = tokens.shape
    width = depth * lax.axis_size("dp")
    blocks, seqs, heads, _ = states.shape
    folded = states.reshape(blocks, seqs, heads, HEAD // 2, LANES)
    folded = jnp.swapaxes(folded, 2, 3).reshape(blocks, seqs * HEAD, LANES)
    columns, owners = lax.axis_size("tp"), lax.axis_size("dp")
    both = ("tp", "dp")
    pairs = [
        [column * owners + owner for column in (first, first + 1) for owner in range(owners)]
        for first in range(0, columns, 2)
    ]
    quads = [
        [column * owners + owner for column in range(first, first + 4) for owner in range(owners)]
        for first in range(0, columns, 4)
    ]
    half, quarter = own_count // 2, own_count // 4
    limits = lengths.reshape(1, -1)
    gathered = exchange(jnp.broadcast_to(tokens, (columns, own_count, depth)), "tp")
    other_out = from_partner(w_out, "tp")
    own_weights = call(
        functools.partial(stack_kernel, 1), bf16(6, depth, LANES), *weights
    )
    other_weights = from_partner(own_weights, "tp")
    packed = call(
        pack_kernel,
        bf16(2 * LANES + half + 16, depth),
        w_out, other_out, tokens, norm_gain,
    )
    packed = from_partner(packed, "dp")
    out_pair = call(functools.partial(stack_kernel, 1), bf16(2, LANES, depth), w_out, other_out)
    out_far = lax.ppermute(out_pair, "tp", [(i, i ^ 2) for i in range(columns)])
    core_own = from_partner(own_weights, "dp")
    core_other = from_partner(other_weights, "dp")
    far = call(
        functools.partial(project_kernel, True),
        bf16(columns, 3 * own_count + 8, LANES),
        gathered, norm_gain, *weights, limits, decay_base, group_gain,
    )
    came = from_partner(far, "dp")
    near = call(
        functools.partial(project_kernel, False),
        bf16(columns, 3 * own_count + 8, LANES),
        gathered, norm_gain, *weights, came,
    )
    arrived = exchange(near, "dp")
    shared, first_states = advance(
        0, width, (2, owners, quarter, LANES), arrived, limits, decay_base, group_gain,
        folded, [other_out],
    )
    shared = exchange(shared.reshape(2 * owners, quarter, LANES), both, pairs)
    product = call(
        functools.partial(out_kernel, 0),
        bf16(columns, quarter, 2 * depth),
        shared.reshape(2, owners, quarter, LANES), w_out, other_out, packed,
        awaited=[other_weights, out_far],
    )
    summed = exchange(product, "tp")
    rows, spread = call(
        settle_kernel,
        (bf16(2, quarter, 2 * depth), bf16(columns, quarter, 2 * depth)),
        summed, tokens, packed,
        awaited=[core_own, core_other],
    )
    gathered = exchange(spread, "tp")
    near = call(
        project_pair_kernel,
        bf16(2, columns, 6 * quarter + 8, LANES),
        gathered, norm_gain, packed, *weights, other_weights, core_own, core_other,
    )
    arrived = exchange(near.reshape(-1, *near.shape[2:]), both, pairs)
    back = from_partner(rows[:, :, depth:], "dp")
    shared, last_states = advance(
        1, width, (4, owners, quarter, LANES), arrived, limits, decay_base, group_gain,
        folded, [],
    )
    shared = exchange(shared.reshape(4 * owners, quarter, LANES), both, quads)
    product = call(
        out_quad_kernel,
        bf16(columns, quarter, depth),
        shared.reshape(4, owners, quarter, LANES), out_pair, out_far,
    )
    summed = exchange(product, "tp")
    own_rows = call(finish_kernel, bf16(own_count, depth), summed, rows, back)
    held = jnp.stack([first_states, last_states])
    new_states = jnp.swapaxes(held.reshape(blocks, seqs, HEAD // 2, heads, LANES), 2, 3)
    return (own_rows, new_states.reshape(states.shape))


def solution(mesh):
    placed = (
        P(("grp", "tp"), "dp"),
        P(("grp", "dp")),
        P(None, "dp"),
        P(None, "dp", "tp"),
        P(None, "dp", "tp"),
        P(None, "dp", "tp"),
        P(None, "dp", "tp"),
        P(None, "dp", "tp"),
        P(None, "dp", "tp"),
        P(None, "tp"),
        P(None, "tp"),
        P(None, "tp", "dp"),
        P(None, ("grp", "dp"), "tp", None),
    )
    return jax.shard_map(
        per_device,
        mesh=mesh,
        in_specs=placed,
        out_specs=(P(("grp", "tp"), "dp"), P(None, ("grp", "dp"), "tp", None)),
        check_vma=False,
    )
```

```python
import functools

import jax
import jax.numpy as jnp
from jax import lax
from jax.experimental import pallas as pl
from jax.experimental.pallas import tpu as pltpu
from jax.sharding import PartitionSpec as P


HEAD = 64
NEW = 4
LANES = 128

norm_epsilon = 1e-06
unit_epsilon = 0.00064
group_epsilon = 0.00064

VMEM = pl.BlockSpec(memory_space=pltpu.VMEM)


def place():
    return lax.rem(lax.axis_index("dp"), 2), lax.rem(lax.axis_index("tp"), 2)


def iota(shape, dim):
    return lax.broadcasted_iota(jnp.int32, shape, dim)


def split_dot(x, ones):
    high = x.astype(jnp.bfloat16)
    low = (x - high.astype(jnp.float32)).astype(jnp.bfloat16)
    return jnp.dot(high, ones, preferred_element_type=jnp.float32) + jnp.dot(
        low, ones, preferred_element_type=jnp.float32
    )


def squares_tail(row):
    pick = iota((8, LANES), 0)
    high = row.astype(jnp.bfloat16).astype(jnp.float32)
    return jnp.where(pick == 0, high, jnp.where(pick == 1, row - high, 0.0)).astype(jnp.bfloat16)


def project_kernel(far, x_ref, gain_ref, *refs):
    out_ref = refs[-1]
    blocks, rows, depth = x_ref.shape
    half = rows // 2
    first_half = place()[0] == (1 if far else 0)
    x = x_ref[...].astype(jnp.float32)
    x = jnp.where(first_half, x[:, :half], x[:, half:]).reshape(blocks * half, depth)
    scaled = (x * gain_ref[0:1, :]).astype(jnp.bfloat16)
    squares = jnp.sum(x * x, -1, keepdims=True)
    eye = iota((half, LANES), 0) == iota((half, LANES), 1)
    for first in range(0, 6, 2):
        pair = jnp.concatenate([refs[first][0], refs[first + 1][0]], 1)
        product = jnp.dot(scaled, pair, preferred_element_type=jnp.float32)
        for side in range(2):
            part = product[:, side * LANES : (side + 1) * LANES].reshape(blocks, half, LANES)
            where = pl.ds((first + side) * half, half)
            if not far:
                part = part + refs[-2][:, where, :].astype(jnp.float32)
            out_ref[:, where, :] = part.astype(jnp.bfloat16)
    for block in range(blocks):
        row = jnp.sum(
            jnp.where(eye, squares[block * half : (block + 1) * half], 0.0), 0, keepdims=True
        )
        if not far:
            came = refs[-2][block, pl.ds(6 * half, 8), :].astype(jnp.float32)
            row = row + came[0:1] + came[1:2]
        out_ref[block, pl.ds(6 * half, 8), :] = squares_tail(row)


def project_pair_kernel(x_ref, gain_ref, packed_ref, *refs):
    *weight_refs, other_ref, core_own_ref, core_other_ref, out_ref = refs
    column = place()[1]
    blocks, rows, both = x_ref.shape
    depth = both // 2
    x = x_ref[...].astype(jnp.float32).reshape(blocks * rows, both)
    core_gain = packed_ref[pl.ds(packed_ref.shape[0] - 16, 16), :].astype(jnp.float32)
    core_gain = core_gain[0:1] + core_gain[1:2] + core_gain[2:3]
    own_scaled = (x[:, :depth] * gain_ref[1:2, :]).astype(jnp.bfloat16)
    core_scaled = (x[:, depth:] * core_gain).astype(jnp.bfloat16)
    squares = jnp.sum(x * x, -1, keepdims=True)
    eye = iota((rows, LANES), 0) == iota((rows, LANES), 1)
    for group in range(2):
        member = jnp.bitwise_xor(column, group)
        for first in range(0, 6, 2):
            if group:
                near = [other_ref[first], other_ref[first + 1]]
                core = [core_other_ref[first], core_other_ref[first + 1]]
            else:
                near = [weight_refs[first][1], weight_refs[first + 1][1]]
                core = [core_own_ref[first], core_own_ref[first + 1]]
            product = jnp.dot(
                own_scaled, jnp.concatenate(near, 1), preferred_element_type=jnp.float32
            ) + jnp.dot(core_scaled, jnp.concatenate(core, 1), preferred_element_type=jnp.float32)
            for side in range(2):
                part = product[:, side * LANES : (side + 1) * LANES]
                out_ref[member, :, pl.ds((first + side) * rows, rows), :] = part.reshape(
                    blocks, rows, LANES
                ).astype(jnp.bfloat16)
        for block in range(blocks):
            row = jnp.sum(
                jnp.where(eye, squares[block * rows : (block + 1) * rows], 0.0), 0, keepdims=True
            )
            out_ref[member, block, pl.ds(6 * rows, 8), :] = squares_tail(row)


def advance_kernel(layer, rows, width, arrived_ref, limits_ref, lines_ref, state_ref, *refs):
    mixed_ref, new_ref, line_ref, read_ref = refs[-4:]
    seqs = rows // NEW
    parts, part_rows = arrived_ref.shape[0], (arrived_ref.shape[1] - 8) // 6
    eye = iota((part_rows, LANES), 0) == iota((part_rows, LANES), 1)
    scaled = []
    for part in range(rows // part_rows):
        outer, core = part // 2, part % 2
        chips = parts * part_rows // rows
        total = arrived_ref[outer * chips * 2 + core].astype(jnp.float32)
        for chip in range(1, chips):
            total += arrived_ref[(outer * chips + chip) * 2 + core].astype(jnp.float32)
        square = total[6 * part_rows : 6 * part_rows + 1] + total[6 * part_rows + 1 : 6 * part_rows + 2]
        square = jnp.sum(jnp.where(eye, square, 0.0), 1, keepdims=True)
        inv_rms = lax.rsqrt(square / width + norm_epsilon)
        scaled.append(
            [inv_rms * total[role * part_rows : (role + 1) * part_rows] for role in range(6)]
        )
    recept, keys, values, decay_pre, rate_pre, gate_pre = [
        jnp.concatenate([part[role] for part in scaled], 0).astype(jnp.bfloat16).astype(jnp.float32)
        for role in range(6)
    ]
    same_head = (iota((LANES, LANES), 0) // HEAD == iota((LANES, LANES), 1) // HEAD).astype(
        jnp.float32
    ).astype(jnp.bfloat16)
    log_rate = lines_ref[layer : layer + 1, :] + decay_pre
    decays = jnp.exp(jax.nn.sigmoid(log_rate) * (-0.6065306597126334))
    rates = jax.nn.sigmoid(rate_pre)
    unit = keys * lax.rsqrt(split_dot(keys * keys, same_head) + unit_epsilon)
    seqs_row = limits_ref[...].astype(jnp.float32)
    of_seq = iota((rows, seqs), 0) // NEW == iota((rows, seqs), 1)
    limit = jnp.sum(jnp.where(of_seq, seqs_row, 0.0), 1, keepdims=True)
    live = (iota((rows, LANES), 0) % NEW).astype(jnp.float32) < limit
    decays = jnp.where(live, decays, 1.0)
    unit = jnp.where(live, unit, 0.0)
    keys = jnp.where(live, keys, 0.0)
    lane = iota((rows, LANES), 1)
    for place, line in enumerate((decays, unit, unit * rates, keys, recept)):
        turned = pltpu.roll(line, HEAD, 1)
        line_ref[2 * place] = jnp.where(lane < HEAD, line, turned)
        line_ref[2 * place + 1] = jnp.where(lane < HEAD, turned, line)
    line_ref[10] = values
    even = iota((8, LANES), 0) % 2 == 0
    block_row, block_lane = iota((HEAD, LANES), 0), iota((HEAD, LANES), 1)
    place_mask = (block_row % 2 == block_lane // HEAD) & (block_row // 2 == block_lane % HEAD // 2)
    parity = (iota((LANES, LANES), 0) % 2 == iota((LANES, LANES), 1) // HEAD).astype(
        jnp.float32
    ).astype(jnp.bfloat16)
    parity_back = (iota((LANES, LANES), 1) % 2 == iota((LANES, LANES), 0) // HEAD).astype(
        jnp.float32
    ).astype(jnp.bfloat16)

    def spread(place, token):
        return jnp.where(
            even, line_ref[2 * place, pl.ds(token, 1), :], line_ref[2 * place + 1, pl.ds(token, 1), :]
        )[None]

    state = [
        state_ref[layer, pl.ds(seq * HEAD, HEAD), :].reshape(8, 8, LANES) for seq in range(seqs)
    ]
    for position in range(NEW):
        tokens = [seq * NEW + position for seq in range(seqs)]
        against = jnp.concatenate(
            [(s * spread(1, t)).reshape(HEAD, LANES) for s, t in zip(state, tokens)], 0
        )
        removed = jnp.dot(
            against.astype(jnp.bfloat16), same_head, preferred_element_type=jnp.float32
        )
        written = jnp.concatenate(
            [jnp.where(place_mask, line_ref[10, pl.ds(t, 1), :], 0.0) for t in tokens], 0
        ).astype(jnp.bfloat16)
        written = jnp.dot(written, parity, preferred_element_type=jnp.float32)
        for seq, t in enumerate(tokens):
            part = slice(seq * HEAD, (seq + 1) * HEAD)
            state[seq] = (
                state[seq] * spread(0, t)
                - removed[part].reshape(8, 8, LANES) * spread(2, t)
                + written[part].reshape(8, 8, LANES) * spread(3, t)
            )
        read = jnp.concatenate(
            [(s * spread(4, t)).reshape(HEAD, LANES) for s, t in zip(state, tokens)], 0
        )
        read = jnp.dot(
            read.astype(jnp.bfloat16), parity_back, preferred_element_type=jnp.float32
        )
        for seq, t in enumerate(tokens):
            part = slice(seq * HEAD, (seq + 1) * HEAD)
            read_ref[pl.ds(t, 1), :] = jnp.sum(
                jnp.where(place_mask, read[part], 0.0), 0, keepdims=True
            )
    for seq in range(seqs):
        new_ref[pl.ds(seq * HEAD, HEAD), :] = state[seq].reshape(HEAD, LANES)
    read = read_ref[...]
    centred = read - split_dot(read, same_head) / HEAD
    variance = split_dot(centred * centred, same_head) / HEAD
    normed = centred * lax.rsqrt(variance + group_epsilon) * lines_ref[2 + layer : 3 + layer, :]
    mixed = jnp.where(live, normed * jax.nn.sigmoid(gate_pre), 0.0)
    members, owners, share, _ = mixed_ref.shape
    for member in range(members):
        for owner in range(owners):
            start = member * (rows // members) + (owner % 2) * share * (share * members < rows)
            mixed_ref[member, owner] = mixed[start : start + share].astype(jnp.bfloat16)


def out_kernel(layer, mixed_ref, own_ref, other_ref, *refs):
    out_ref = refs[-1]
    _, blocks, rows, _ = mixed_ref.shape
    depth = own_ref.shape[2]
    first = place()[1] == 0
    sides = [(own_ref[layer], other_ref[layer])]
    if layer == 0:
        sides.append((refs[0][pl.ds(0, LANES), :], refs[0][pl.ds(LANES, LANES), :]))
    for side, (own, other) in enumerate(sides):
        total = 0.0
        for member, matrix in enumerate(
            (jnp.where(first, own, other), jnp.where(first, other, own))
        ):
            lines = mixed_ref[member].astype(jnp.float32).reshape(blocks * rows, LANES)
            total += jnp.dot(
                lines.astype(jnp.bfloat16), matrix, preferred_element_type=jnp.float32
            )
        out_ref[:, :, pl.ds(side * depth, depth)] = total.reshape(blocks, rows, depth).astype(
            jnp.bfloat16
        )


def join_kernel(first_ref, second_ref, out_ref):
    out_ref[...] = jnp.concatenate([first_ref[...], second_ref[...]], 0)


def stack_kernel(layer, *refs):
    for index, ref in enumerate(refs[:-1]):
        refs[-1][index] = ref[layer]


def pack_kernel(own_ref, other_ref, tokens_ref, gain_ref, out_ref):
    quarter = tokens_ref.shape[0] // 4
    out_ref[pl.ds(0, LANES), :] = own_ref[0]
    out_ref[pl.ds(LANES, LANES), :] = other_ref[0]
    lines = []
    for member in range(2):
        near = tokens_ref[pl.ds(member * 2 * quarter, 2 * quarter), :].astype(jnp.float32)
        lines.append(jnp.where(place()[0] == 0, near[quarter:], near[:quarter]))
    out_ref[pl.ds(2 * LANES, 2 * quarter), :] = jnp.concatenate(lines, 0).astype(jnp.bfloat16)
    rest = gain_ref[1:2, :]
    pick = iota((16, rest.shape[1]), 0)
    lines = jnp.zeros(pick.shape, jnp.float32)
    for index in range(3):
        term = rest.astype(jnp.bfloat16).astype(jnp.float32)
        lines = jnp.where(pick == index, term, lines)
        rest = rest - term
    out_ref[pl.ds(2 * LANES + 2 * quarter, 16), :] = lines.astype(jnp.bfloat16)


def settle_kernel(summed_ref, tokens_ref, packed_ref, *refs):
    rows_ref, spread_ref = refs[-2:]
    columns, rows, _ = summed_ref.shape
    first = place()[0] == 0
    for member in range(2):
        total = summed_ref[member].astype(jnp.float32)
        for column in range(member + 2, columns, 2):
            total += summed_ref[column].astype(jnp.float32)
        near = tokens_ref[pl.ds(member * 2 * rows, 2 * rows), :].astype(jnp.float32)
        near = jnp.where(first, near[:rows], near[rows:])
        core = packed_ref[pl.ds(2 * LANES, 2 * rows), :].astype(jnp.float32)
        core = core[member * rows : (member + 1) * rows]
        total = (total + jnp.concatenate([near, core], 1)).astype(jnp.bfloat16)
        rows_ref[member] = total
        for column in range(member, columns, 2):
            spread_ref[column] = total


def finish_kernel(summed_ref, rows_ref, back_ref, out_ref):
    columns, half, depth = summed_ref.shape
    first = place()[0] == 0
    for member in range(2):
        total = summed_ref[member].astype(jnp.float32)
        for column in range(member + 2, columns, 2):
            total += summed_ref[column].astype(jnp.float32)
        near = rows_ref[member].astype(jnp.float32)[:, :depth]
        core = back_ref[member].astype(jnp.float32)
        held = jnp.concatenate([jnp.where(first, near, core), jnp.where(first, core, near)], 0)
        out_ref[pl.ds(member * half, half), :] = (total + held).astype(jnp.bfloat16)


def params():
    return {
        "compiler_params": pltpu.CompilerParams(vmem_limit_bytes=24 * 2**20),
        "cost_estimate": pl.CostEstimate(
            flops=10**8, bytes_accessed=2 * 10**6, transcendentals=0
        ),
    }


def call(kernel, outs, *operands, awaited=()):
    return pl.pallas_call(
        kernel,
        out_shape=outs,
        in_specs=[VMEM] * len(operands)
        + [pl.BlockSpec(memory_space=pl.ANY)] * len(awaited),
        out_specs=jax.tree.map(lambda _: VMEM, outs),
        **params(),
    )(*operands, *awaited)


def bf16(*shape):
    return jax.ShapeDtypeStruct(shape, jnp.bfloat16)


def advance(layer, width, shared, arrived, limits, lines, states, awaited):
    rows = limits.shape[1] * NEW
    return pl.pallas_call(
        functools.partial(advance_kernel, layer, rows, width),
        out_shape=(bf16(*shared), jax.ShapeDtypeStruct(states.shape[1:], jnp.float32)),
        in_specs=[VMEM] * 4 + [pl.BlockSpec(memory_space=pl.ANY)] * len(awaited),
        out_specs=(VMEM, VMEM),
        scratch_shapes=[
            pltpu.VMEM((11, rows, LANES), jnp.float32),
            pltpu.VMEM((rows, LANES), jnp.float32),
        ],
        **params(),
    )(arrived, limits, lines, states, *awaited)


def exchange(x, axis, groups=None):
    return lax.all_to_all(x, axis, 0, 0, tiled=True, axis_index_groups=groups)


def from_partner(x, axis):
    return lax.ppermute(x, axis, [(i, i ^ 1) for i in range(lax.axis_size(axis))])


def per_device(
    tokens,
    lengths,
    norm_gain,
    w_recept,
    w_keys,
    w_values,
    w_decay,
    w_rate,
    w_gate,
    decay_base,
    group_gain,
    w_out,
    states,
):
    weights = (w_recept, w_keys, w_values, w_decay, w_rate, w_gate)
    own_count, depth = tokens.shape
    width = depth * lax.axis_size("dp")
    blocks, seqs, heads, _ = states.shape
    folded = states.reshape(blocks, seqs, heads, HEAD // 2, LANES)
    folded = jnp.swapaxes(folded, 2, 3).reshape(blocks, seqs * HEAD, LANES)
    columns, owners = lax.axis_size("tp"), lax.axis_size("dp")
    both = ("tp", "dp")
    pairs = [
        [column * owners + owner for column in (first, first + 1) for owner in range(owners)]
        for first in range(0, columns, 2)
    ]
    half, quarter = own_count // 2, own_count // 4
    limits = lengths.reshape(1, -1)
    gathered = exchange(jnp.broadcast_to(tokens, (columns, own_count, depth)), "tp")
    other_out = from_partner(w_out, "tp")
    own_weights = call(
        functools.partial(stack_kernel, 1), bf16(6, depth, LANES), *weights
    )
    other_weights = from_partner(own_weights, "tp")
    lines = call(
        join_kernel,
        jax.ShapeDtypeStruct((4, decay_base.shape[1]), jnp.float32),
        decay_base, group_gain,
    )
    packed = call(
        pack_kernel,
        bf16(2 * LANES + half + 16, depth),
        w_out, other_out, tokens, norm_gain,
    )
    packed = from_partner(packed, "dp")
    core_own = from_partner(own_weights, "dp")
    core_other = from_partner(other_weights, "dp")
    far = call(
        functools.partial(project_kernel, True),
        bf16(columns, 3 * own_count + 8, LANES),
        gathered, norm_gain, *weights,
        awaited=[core_own],
    )
    came = from_partner(far, "dp")
    near = call(
        functools.partial(project_kernel, False),
        bf16(columns, 3 * own_count + 8, LANES),
        gathered, norm_gain, *weights, came,
    )
    arrived = exchange(near, "dp")
    shared, first_states = advance(
        0, width, (2, owners, quarter, LANES), arrived, limits, lines, folded, [packed],
    )
    shared = exchange(shared.reshape(2 * owners, quarter, LANES), both, pairs)
    product = call(
        functools.partial(out_kernel, 0),
        bf16(columns, quarter, 2 * depth),
        shared.reshape(2, owners, quarter, LANES), w_out, other_out, packed,
        awaited=[core_other],
    )
    summed = exchange(product, "tp")
    rows, spread = call(
        settle_kernel,
        (bf16(2, quarter, 2 * depth), bf16(columns, quarter, 2 * depth)),
        summed, tokens, packed,
    )
    gathered = exchange(spread, "tp")
    near = call(
        project_pair_kernel,
        bf16(2, columns, 6 * quarter + 8, LANES),
        gathered, norm_gain, packed, *weights, other_weights, core_own, core_other,
    )
    arrived = exchange(near.reshape(-1, *near.shape[2:]), both, pairs)
    back = from_partner(rows[:, :, depth:], "dp")
    shared, last_states = advance(
        1, width, (2, owners, half, LANES), arrived, limits, lines, folded, [],
    )
    shared = exchange(shared.reshape(2 * owners, half, LANES), both, pairs)
    product = call(
        functools.partial(out_kernel, 1),
        bf16(columns, half, depth),
        shared.reshape(2, owners, half, LANES), w_out, other_out,
    )
    summed = exchange(product, "tp")
    own_rows = call(finish_kernel, bf16(own_count, depth), summed, rows, back)
    held = jnp.stack([first_states, last_states])
    new_states = jnp.swapaxes(held.reshape(blocks, seqs, HEAD // 2, heads, LANES), 2, 3)
    return (own_rows, new_states.reshape(states.shape))


def solution(mesh):
    placed = (
        P(("grp", "tp"), "dp"),
        P(("grp", "dp")),
        P(None, "dp"),
        P(None, "dp", "tp"),
        P(None, "dp", "tp"),
        P(None, "dp", "tp"),
        P(None, "dp", "tp"),
        P(None, "dp", "tp"),
        P(None, "dp", "tp"),
        P(None, "tp"),
        P(None, "tp"),
        P(None, "tp", "dp"),
        P(None, ("grp", "dp"), "tp", None),
    )
    return jax.shard_map(
        per_device,
        mesh=mesh,
        in_specs=placed,
        out_specs=(P(("grp", "tp"), "dp"), P(None, ("grp", "dp"), "tp", None)),
        check_vma=False,
    )
```

```python
import functools

import jax
import jax.numpy as jnp
from jax import lax
from jax.experimental import pallas as pl
from jax.experimental.pallas import tpu as pltpu
from jax.sharding import PartitionSpec as P


HEAD = 64
NEW = 4
LANES = 128

norm_epsilon = 1e-06
unit_epsilon = 0.00064
group_epsilon = 0.00064

VMEM = pl.BlockSpec(memory_space=pltpu.VMEM)


def place():
    return lax.rem(lax.axis_index("dp"), 2), lax.rem(lax.axis_index("tp"), 2)


def iota(shape, dim):
    return lax.broadcasted_iota(jnp.int32, shape, dim)


def split_dot(x, ones):
    high = x.astype(jnp.bfloat16)
    low = (x - high.astype(jnp.float32)).astype(jnp.bfloat16)
    return jnp.dot(high, ones, preferred_element_type=jnp.float32) + jnp.dot(
        low, ones, preferred_element_type=jnp.float32
    )


def squares_tail(row):
    pick = iota((8, LANES), 0)
    high = row.astype(jnp.bfloat16).astype(jnp.float32)
    return jnp.where(pick == 0, high, jnp.where(pick == 1, row - high, 0.0)).astype(jnp.bfloat16)


def project_kernel(far, x_ref, gain_ref, *refs):
    out_ref = refs[-1]
    blocks, rows, depth = x_ref.shape
    half = rows // 2
    first_half = place()[0] == (1 if far else 0)
    x = x_ref[...].astype(jnp.float32)
    x = jnp.where(first_half, x[:, :half], x[:, half:]).reshape(blocks * half, depth)
    scaled = (x * gain_ref[0:1, :]).astype(jnp.bfloat16)
    squares = jnp.sum(x * x, -1, keepdims=True)
    eye = iota((half, LANES), 0) == iota((half, LANES), 1)
    for first in range(0, 6, 2):
        pair = jnp.concatenate([refs[first][0], refs[first + 1][0]], 1)
        product = jnp.dot(scaled, pair, preferred_element_type=jnp.float32)
        for side in range(2):
            part = product[:, side * LANES : (side + 1) * LANES].reshape(blocks, half, LANES)
            where = pl.ds((first + side) * half, half)
            if not far:
                part = part + refs[-2][:, where, :].astype(jnp.float32)
            out_ref[:, where, :] = part.astype(jnp.bfloat16)
    for block in range(blocks):
        row = jnp.sum(
            jnp.where(eye, squares[block * half : (block + 1) * half], 0.0), 0, keepdims=True
        )
        if not far:
            came = refs[-2][block, pl.ds(6 * half, 8), :].astype(jnp.float32)
            row = row + came[0:1] + came[1:2]
        out_ref[block, pl.ds(6 * half, 8), :] = squares_tail(row)


def project_pair_kernel(x_ref, gain_ref, packed_ref, *refs):
    *weight_refs, other_ref, core_own_ref, core_other_ref, out_ref = refs
    column = place()[1]
    blocks, rows, both = x_ref.shape
    depth = both // 2
    x = x_ref[...].astype(jnp.float32).reshape(blocks * rows, both)
    core_gain = packed_ref[pl.ds(packed_ref.shape[0] - 16, 16), :].astype(jnp.float32)
    core_gain = core_gain[0:1] + core_gain[1:2] + core_gain[2:3]
    own_scaled = (x[:, :depth] * gain_ref[1:2, :]).astype(jnp.bfloat16)
    core_scaled = (x[:, depth:] * core_gain).astype(jnp.bfloat16)
    squares = jnp.sum(x * x, -1, keepdims=True)
    eye = iota((rows, LANES), 0) == iota((rows, LANES), 1)
    for group in range(2):
        member = jnp.bitwise_xor(column, group)
        for first in range(0, 6, 2):
            if group:
                near = [other_ref[first], other_ref[first + 1]]
                core = [core_other_ref[first], core_other_ref[first + 1]]
            else:
                near = [weight_refs[first][1], weight_refs[first + 1][1]]
                core = [core_own_ref[first], core_own_ref[first + 1]]
            product = jnp.dot(
                own_scaled, jnp.concatenate(near, 1), preferred_element_type=jnp.float32
            ) + jnp.dot(core_scaled, jnp.concatenate(core, 1), preferred_element_type=jnp.float32)
            for side in range(2):
                part = product[:, side * LANES : (side + 1) * LANES]
                out_ref[member, :, pl.ds((first + side) * rows, rows), :] = part.reshape(
                    blocks, rows, LANES
                ).astype(jnp.bfloat16)
        for block in range(blocks):
            row = jnp.sum(
                jnp.where(eye, squares[block * rows : (block + 1) * rows], 0.0), 0, keepdims=True
            )
            out_ref[member, block, pl.ds(6 * rows, 8), :] = squares_tail(row)


def advance_kernel(layer, rows, width, arrived_ref, limits_ref, lines_ref, state_ref, *refs):
    mixed_ref, new_ref, line_ref, read_ref = refs[-4:]
    seqs = rows // NEW
    parts, part_rows = arrived_ref.shape[0], (arrived_ref.shape[1] - 8) // 6
    eye = iota((part_rows, LANES), 0) == iota((part_rows, LANES), 1)
    scaled = []
    for part in range(rows // part_rows):
        outer, core = part // 2, part % 2
        chips = parts * part_rows // rows
        total = arrived_ref[outer * chips * 2 + core].astype(jnp.float32)
        for chip in range(1, chips):
            total += arrived_ref[(outer * chips + chip) * 2 + core].astype(jnp.float32)
        square = total[6 * part_rows : 6 * part_rows + 1] + total[6 * part_rows + 1 : 6 * part_rows + 2]
        square = jnp.sum(jnp.where(eye, square, 0.0), 1, keepdims=True)
        inv_rms = lax.rsqrt(square / width + norm_epsilon)
        scaled.append(
            [inv_rms * total[role * part_rows : (role + 1) * part_rows] for role in range(6)]
        )
    recept, keys, values, decay_pre, rate_pre, gate_pre = [
        jnp.concatenate([part[role] for part in scaled], 0).astype(jnp.bfloat16).astype(jnp.float32)
        for role in range(6)
    ]
    same_head = (iota((LANES, LANES), 0) // HEAD == iota((LANES, LANES), 1) // HEAD).astype(
        jnp.float32
    ).astype(jnp.bfloat16)
    log_rate = lines_ref[layer : layer + 1, :] + decay_pre
    decays = jnp.exp(jax.nn.sigmoid(log_rate) * (-0.6065306597126334))
    rates = jax.nn.sigmoid(rate_pre)
    unit = keys * lax.rsqrt(split_dot(keys * keys, same_head) + unit_epsilon)
    live = (iota((rows, LANES), 0) % NEW).astype(jnp.float32) < limits_ref[...]
    decays = jnp.where(live, decays, 1.0)
    unit = jnp.where(live, unit, 0.0)
    keys = jnp.where(live, keys, 0.0)
    lane = iota((rows, LANES), 1)
    for place, line in enumerate((decays, unit, unit * rates, keys, recept)):
        turned = pltpu.roll(line, HEAD, 1)
        line_ref[2 * place] = jnp.where(lane < HEAD, line, turned)
        line_ref[2 * place + 1] = jnp.where(lane < HEAD, turned, line)
    line_ref[10] = values
    even = iota((8, LANES), 0) % 2 == 0
    block_row, block_lane = iota((HEAD, LANES), 0), iota((HEAD, LANES), 1)
    place_mask = (block_row % 2 == block_lane // HEAD) & (block_row // 2 == block_lane % HEAD // 2)
    parity = (iota((LANES, LANES), 0) % 2 == iota((LANES, LANES), 1) // HEAD).astype(
        jnp.float32
    ).astype(jnp.bfloat16)
    parity_back = (iota((LANES, LANES), 1) % 2 == iota((LANES, LANES), 0) // HEAD).astype(
        jnp.float32
    ).astype(jnp.bfloat16)

    def spread(place, token):
        return jnp.where(
            even, line_ref[2 * place, pl.ds(token, 1), :], line_ref[2 * place + 1, pl.ds(token, 1), :]
        )[None]

    state = [
        state_ref[layer, pl.ds(seq * HEAD, HEAD), :].reshape(8, 8, LANES) for seq in range(seqs)
    ]
    for position in range(NEW):
        tokens = [seq * NEW + position for seq in range(seqs)]
        against = jnp.concatenate(
            [(s * spread(1, t)).reshape(HEAD, LANES) for s, t in zip(state, tokens)], 0
        )
        removed = jnp.dot(
            against.astype(jnp.bfloat16), same_head, preferred_element_type=jnp.float32
        )
        written = jnp.concatenate(
            [jnp.where(place_mask, line_ref[10, pl.ds(t, 1), :], 0.0) for t in tokens], 0
        ).astype(jnp.bfloat16)
        written = jnp.dot(written, parity, preferred_element_type=jnp.float32)
        for seq, t in enumerate(tokens):
            part = slice(seq * HEAD, (seq + 1) * HEAD)
            state[seq] = (
                state[seq] * spread(0, t)
                - removed[part].reshape(8, 8, LANES) * spread(2, t)
                + written[part].reshape(8, 8, LANES) * spread(3, t)
            )
        read = jnp.concatenate(
            [(s * spread(4, t)).reshape(HEAD, LANES) for s, t in zip(state, tokens)], 0
        )
        read = jnp.dot(
            read.astype(jnp.bfloat16), parity_back, preferred_element_type=jnp.float32
        )
        for seq, t in enumerate(tokens):
            part = slice(seq * HEAD, (seq + 1) * HEAD)
            read_ref[pl.ds(t, 1), :] = jnp.sum(
                jnp.where(place_mask, read[part], 0.0), 0, keepdims=True
            )
    for seq in range(seqs):
        new_ref[pl.ds(seq * HEAD, HEAD), :] = state[seq].reshape(HEAD, LANES)
    read = read_ref[...]
    centred = read - split_dot(read, same_head) / HEAD
    variance = split_dot(centred * centred, same_head) / HEAD
    normed = centred * lax.rsqrt(variance + group_epsilon) * lines_ref[2 + layer : 3 + layer, :]
    mixed = jnp.where(live, normed * jax.nn.sigmoid(gate_pre), 0.0)
    members, owners, share, _ = mixed_ref.shape
    for member in range(members):
        for owner in range(owners):
            start = member * (rows // members) + (owner % 2) * share * (share * members < rows)
            mixed_ref[member, owner] = mixed[start : start + share].astype(jnp.bfloat16)


def out_kernel(layer, mixed_ref, own_ref, other_ref, *refs):
    out_ref = refs[-1]
    _, blocks, rows, _ = mixed_ref.shape
    depth = own_ref.shape[2]
    first = place()[1] == 0
    sides = [(own_ref[layer], other_ref[layer])]
    if layer == 0:
        sides.append((refs[0][pl.ds(0, LANES), :], refs[0][pl.ds(LANES, LANES), :]))
    for side, (own, other) in enumerate(sides):
        total = 0.0
        for member, matrix in enumerate(
            (jnp.where(first, own, other), jnp.where(first, other, own))
        ):
            lines = mixed_ref[member].astype(jnp.float32).reshape(blocks * rows, LANES)
            total += jnp.dot(
                lines.astype(jnp.bfloat16), matrix, preferred_element_type=jnp.float32
            )
        out_ref[:, :, pl.ds(side * depth, depth)] = total.reshape(blocks, rows, depth).astype(
            jnp.bfloat16
        )


def join_kernel(first_ref, second_ref, lengths_ref, lines_ref, limits_ref):
    lines_ref[...] = jnp.concatenate([first_ref[...], second_ref[...]], 0)
    rows = limits_ref.shape[0]
    of_seq = iota((rows, rows // NEW), 0) // NEW == iota((rows, rows // NEW), 1)
    limit = jnp.where(of_seq, lengths_ref[...].astype(jnp.float32), 0.0)
    limits_ref[...] = jnp.broadcast_to(jnp.sum(limit, 1, keepdims=True), limits_ref.shape)


def store_kernel(states_ref, *refs):
    refs[-1][0] = states_ref[...]


def store(layer, states, held):
    return pl.pallas_call(
        store_kernel,
        grid=(1,),
        out_shape=jax.ShapeDtypeStruct((2, *states.shape), states.dtype),
        in_specs=[VMEM] + [pl.BlockSpec(memory_space=pl.ANY)] * (layer > 0),
        out_specs=pl.BlockSpec((1, *states.shape), lambda i: (layer, 0, 0)),
        input_output_aliases={1: 0} if layer else {},
        **params(),
    )(states, *([held] if layer else []))


def stack_kernel(layer, *refs):
    for index, ref in enumerate(refs[:-1]):
        refs[-1][index] = ref[layer]


def pack_kernel(own_ref, other_ref, tokens_ref, gain_ref, out_ref):
    quarter = tokens_ref.shape[0] // 4
    out_ref[pl.ds(0, LANES), :] = own_ref[0]
    out_ref[pl.ds(LANES, LANES), :] = other_ref[0]
    lines = []
    for member in range(2):
        near = tokens_ref[pl.ds(member * 2 * quarter, 2 * quarter), :].astype(jnp.float32)
        lines.append(jnp.where(place()[0] == 0, near[quarter:], near[:quarter]))
    out_ref[pl.ds(2 * LANES, 2 * quarter), :] = jnp.concatenate(lines, 0).astype(jnp.bfloat16)
    rest = gain_ref[1:2, :]
    pick = iota((16, rest.shape[1]), 0)
    lines = jnp.zeros(pick.shape, jnp.float32)
    for index in range(3):
        term = rest.astype(jnp.bfloat16).astype(jnp.float32)
        lines = jnp.where(pick == index, term, lines)
        rest = rest - term
    out_ref[pl.ds(2 * LANES + 2 * quarter, 16), :] = lines.astype(jnp.bfloat16)


def settle_kernel(summed_ref, tokens_ref, packed_ref, *refs):
    rows_ref, spread_ref = refs[-2:]
    columns, rows, _ = summed_ref.shape
    first = place()[0] == 0
    for member in range(2):
        total = summed_ref[member].astype(jnp.float32)
        for column in range(member + 2, columns, 2):
            total += summed_ref[column].astype(jnp.float32)
        near = tokens_ref[pl.ds(member * 2 * rows, 2 * rows), :].astype(jnp.float32)
        near = jnp.where(first, near[:rows], near[rows:])
        core = packed_ref[pl.ds(2 * LANES, 2 * rows), :].astype(jnp.float32)
        core = core[member * rows : (member + 1) * rows]
        total = (total + jnp.concatenate([near, core], 1)).astype(jnp.bfloat16)
        rows_ref[member] = total
        for column in range(member, columns, 2):
            spread_ref[column] = total


def finish_kernel(summed_ref, rows_ref, back_ref, out_ref):
    columns, half, depth = summed_ref.shape
    first = place()[0] == 0
    for member in range(2):
        total = summed_ref[member].astype(jnp.float32)
        for column in range(member + 2, columns, 2):
            total += summed_ref[column].astype(jnp.float32)
        near = rows_ref[member].astype(jnp.float32)[:, :depth]
        core = back_ref[member].astype(jnp.float32)
        held = jnp.concatenate([jnp.where(first, near, core), jnp.where(first, core, near)], 0)
        out_ref[pl.ds(member * half, half), :] = (total + held).astype(jnp.bfloat16)


def params():
    return {
        "compiler_params": pltpu.CompilerParams(vmem_limit_bytes=24 * 2**20),
        "cost_estimate": pl.CostEstimate(
            flops=10**8, bytes_accessed=2 * 10**6, transcendentals=0
        ),
    }


def call(kernel, outs, *operands, awaited=()):
    return pl.pallas_call(
        kernel,
        out_shape=outs,
        in_specs=[VMEM] * len(operands)
        + [pl.BlockSpec(memory_space=pl.ANY)] * len(awaited),
        out_specs=jax.tree.map(lambda _: VMEM, outs),
        **params(),
    )(*operands, *awaited)


def bf16(*shape):
    return jax.ShapeDtypeStruct(shape, jnp.bfloat16)


def advance(layer, width, shared, arrived, limits, lines, states, awaited):
    rows = limits.shape[0]
    return pl.pallas_call(
        functools.partial(advance_kernel, layer, rows, width),
        out_shape=(bf16(*shared), jax.ShapeDtypeStruct(states.shape[1:], jnp.float32)),
        in_specs=[VMEM] * 4 + [pl.BlockSpec(memory_space=pl.ANY)] * len(awaited),
        out_specs=(VMEM, VMEM),
        scratch_shapes=[
            pltpu.VMEM((11, rows, LANES), jnp.float32),
            pltpu.VMEM((rows, LANES), jnp.float32),
        ],
        **params(),
    )(arrived, limits, lines, states, *awaited)


def exchange(x, axis, groups=None):
    return lax.all_to_all(x, axis, 0, 0, tiled=True, axis_index_groups=groups)


def from_partner(x, axis):
    return lax.ppermute(x, axis, [(i, i ^ 1) for i in range(lax.axis_size(axis))])


def per_device(
    tokens,
    lengths,
    norm_gain,
    w_recept,
    w_keys,
    w_values,
    w_decay,
    w_rate,
    w_gate,
    decay_base,
    group_gain,
    w_out,
    states,
):
    weights = (w_recept, w_keys, w_values, w_decay, w_rate, w_gate)
    own_count, depth = tokens.shape
    width = depth * lax.axis_size("dp")
    blocks, seqs, heads, _ = states.shape
    folded = states.reshape(blocks, seqs, heads, HEAD // 2, LANES)
    folded = jnp.swapaxes(folded, 2, 3).reshape(blocks, seqs * HEAD, LANES)
    columns, owners = lax.axis_size("tp"), lax.axis_size("dp")
    both = ("tp", "dp")
    pairs = [
        [column * owners + owner for column in (first, first + 1) for owner in range(owners)]
        for first in range(0, columns, 2)
    ]
    half, quarter = own_count // 2, own_count // 4
    gathered = exchange(jnp.broadcast_to(tokens, (columns, own_count, depth)), "tp")
    other_out = from_partner(w_out, "tp")
    own_weights = call(
        functools.partial(stack_kernel, 1), bf16(6, depth, LANES), *weights
    )
    other_weights = from_partner(own_weights, "tp")
    lines, limits = call(
        join_kernel,
        (
            jax.ShapeDtypeStruct((4, LANES), jnp.float32),
            jax.ShapeDtypeStruct((own_count, LANES), jnp.float32),
        ),
        decay_base, group_gain, lengths.reshape(1, -1),
    )
    packed = call(
        pack_kernel,
        bf16(2 * LANES + half + 16, depth),
        w_out, other_out, tokens, norm_gain,
    )
    packed = from_partner(packed, "dp")
    core_own = from_partner(own_weights, "dp")
    core_other = from_partner(other_weights, "dp")
    far = call(
        functools.partial(project_kernel, True),
        bf16(columns, 3 * own_count + 8, LANES),
        gathered, norm_gain, *weights,
    )
    came = from_partner(far, "dp")
    near = call(
        functools.partial(project_kernel, False),
        bf16(columns, 3 * own_count + 8, LANES),
        gathered, norm_gain, *weights, came,
    )
    arrived = exchange(near, "dp")
    shared, first_states = advance(
        0, width, (2, owners, quarter, LANES), arrived, limits, lines, folded, [packed],
    )
    shared = exchange(shared.reshape(2 * owners, quarter, LANES), both, pairs)
    product = call(
        functools.partial(out_kernel, 0),
        bf16(columns, quarter, 2 * depth),
        shared.reshape(2, owners, quarter, LANES), w_out, other_out, packed,
    )
    summed = exchange(product, "tp")
    held = store(0, first_states, None)
    rows, spread = call(
        settle_kernel,
        (bf16(2, quarter, 2 * depth), bf16(columns, quarter, 2 * depth)),
        summed, tokens, packed,
        awaited=[core_own, core_other],
    )
    gathered = exchange(spread, "tp")
    near = call(
        project_pair_kernel,
        bf16(2, columns, 6 * quarter + 8, LANES),
        gathered, norm_gain, packed, *weights, other_weights, core_own, core_other,
    )
    arrived = exchange(near.reshape(-1, *near.shape[2:]), both, pairs)
    back = from_partner(rows[:, :, depth:], "dp")
    shared, last_states = advance(
        1, width, (2, owners, half, LANES), arrived, limits, lines, folded, [],
    )
    shared = exchange(shared.reshape(2 * owners, half, LANES), both, pairs)
    product = call(
        functools.partial(out_kernel, 1),
        bf16(columns, half, depth),
        shared.reshape(2, owners, half, LANES), w_out, other_out,
    )
    summed = exchange(product, "tp")
    own_rows = call(finish_kernel, bf16(own_count, depth), summed, rows, back)
    held = store(1, last_states, held)
    new_states = jnp.swapaxes(held.reshape(blocks, seqs, HEAD // 2, heads, LANES), 2, 3)
    return (own_rows, new_states.reshape(states.shape))


def solution(mesh):
    placed = (
        P(("grp", "tp"), "dp"),
        P(("grp", "dp")),
        P(None, "dp"),
        P(None, "dp", "tp"),
        P(None, "dp", "tp"),
        P(None, "dp", "tp"),
        P(None, "dp", "tp"),
        P(None, "dp", "tp"),
        P(None, "dp", "tp"),
        P(None, "tp"),
        P(None, "tp"),
        P(None, "tp", "dp"),
        P(None, ("grp", "dp"), "tp", None),
    )
    return jax.shard_map(
        per_device,
        mesh=mesh,
        in_specs=placed,
        out_specs=(P(("grp", "tp"), "dp"), P(None, ("grp", "dp"), "tp", None)),
        check_vma=False,
    )
```
